32 devices in a mesh: ep: 8 (over z, x), tp: 4 (over y, core).
Axes of the slice: x: 2, y: 2, z: 4, core: 2. Of those that a mesh axis runs over, the one named last changes fastest.
Arguments:
- query_rows: bfloat16 [4096, 3072], P('ep', 'tp'), may hold values from -6 to 6
- key_rows: bfloat16 [4096, 1024], P('ep', 'tp'), may hold values from -6 to 6
- value_rows: bfloat16 [4096, 1024], P('ep', 'tp'), may hold values from -6 to 6
- query_gain: float32 [48, 64], P('tp'), may hold values from 0.4 to 48
- key_gain: float32 [16, 64], P('tp'), may hold values from 0.1 to 1.9
- sink_logits: float32 [48], P('tp'), may hold values from 1 to 6
- out_weight: bfloat16 [3072, 2048], P('tp'), may hold values from -0.109375 to 0.109375
- expert_input: bfloat16 [4096, 2048], P(('ep', 'tp')), may hold values from -6 to 6
- expert_gain: float32 [2048], replicated, may hold values from 0.1 to 1.9
- routes: int32 [4096, 2], P(('ep', 'tp')), may hold values from 0 to 31, all different within a row; in each aligned block of 128 rows (0 to 127, 128 to 255, ...) at most 12 rows name the same one
- route_logits: float32 [4096, 2], P(('ep', 'tp')), may hold values from -6 to 6
- gate_weight: bfloat16 [32, 2048, 2048], P('ep', None, 'tp'), may hold values from -0.375 to 0.375
- up_weight: bfloat16 [32, 2048, 2048], P('ep', None, 'tp'), may hold values from -0.375 to 0.375
- down_weight: bfloat16 [32, 2048, 2048], P('ep', 'tp'), may hold values from -0.01953125 to 0.01953125
Outputs:
- attended: bfloat16 [4096, 2048], P(('ep', 'tp'))
- expert_mix: bfloat16 [4096, 2048], P(('ep', 'tp'))
The draws below stay inside these ranges and needn't reach their ends.
Inputs may be any that keep to these rules, and one draw needn't show every extreme that they name: `routes`: each row names 2 different experts; in the rows of one device no expert is named more than 12 times, and in some device one expert is named exactly 12 times.
All inputs are finite; a program needn't handle non-finite values.
Results may differ from the reference program's by a relative error of at most 0.017.
The reference program's roundings to bfloat16 on the way count: a program that leaves them out, or rounds other values in their place, can miss the bound.
Values may be sent and summed in bfloat16 or wider, within the bound.
A program may use at most 128 MiB of HBM per device.

```python
import math
import jax
import jax.numpy as jnp
import numpy as np
from jax import lax

WIDTH = 2048
QHEADS = 48
KVHEADS = 16
HEADDIM = 64
FFN = 2048
EXPERTS = 32
TOPK = 2
WINDOW = 128
TOKENS = 4096
ROWS_DEV = 128
CAP = 12
N_TP = 4


def draw_query_gain(key, part):
    head_key, spread_key = jax.random.split(key)
    head_scale = jnp.exp(jax.random.uniform(head_key, (QHEADS, 1), jnp.float32, math.log(0.7), math.log(3.0)))
    spread = 1.0 + 0.18 * jax.random.uniform(spread_key, (QHEADS, HEADDIM), jnp.float32, -1.0, 1.0)
    return head_scale * spread


def levels(stream_key, dims, pieces, least, high):
    factor_of = 1.0
    for dim, parts in pieces:
        draws = jax.random.uniform(jax.random.fold_in(jax.random.fold_in(stream_key, 6), dim), (parts,), jnp.float32, least / len(pieces), high / len(pieces))
        factor_of = factor_of * jnp.repeat(jnp.exp(draws), dims[dim] // parts).reshape((-1,) + (1,) * (len(dims) - 1 - dim))
    return factor_of


def assign_block(own_key, own, number, rows, number_of, top, bound, lean):
    sequence = jax.random.permutation(own_key, number_of)
    packed, ordinary = load_shares(number_of, rows * top, bound, lean, True), load_shares(number_of, rows * top, bound, lean, False)
    places = jnp.arange(number_of)

    def named(lengths, rotation):
        used = int((lengths > 0).sum())
        fixed = max(1, used // 4)
        passed = fixed + (places - fixed + rotation * (used - fixed)) % max(1, number_of - fixed)
        return jnp.zeros((number_of,), jnp.int32).at[sequence[jnp.where(places < fixed, places, passed)]].set(jnp.asarray(lengths, jnp.int32))

    lengths = jnp.where(number % 4 == 0, named(packed, number // 4), named(ordinary, number - number // 4 - 1))
    mixed = jax.random.permutation(jax.random.fold_in(own, 3), number_of)
    source_of, receiver = mixed[0:number_of // 2 * 2:2], mixed[1:number_of // 2 * 2:2]
    room = jnp.minimum(lengths[source_of] - 1, bound - lengths[receiver]) // 2
    room = jnp.where((source_of == sequence[0]) | (receiver == sequence[0]) | (lengths[receiver] == 0), 0, jnp.maximum(room, 0))
    passed = jax.random.randint(jax.random.fold_in(own, 4), (number_of // 2,), 0, 1 << 20) % (room + 1)
    lengths = lengths.at[source_of].add(-passed).at[receiver].add(passed)
    labels = jnp.searchsorted(jnp.cumsum(lengths), jnp.arange(rows * top), side="right").astype(jnp.int32)
    table = labels.reshape(top, rows).T
    table = table[jax.random.permutation(jax.random.fold_in(own, 1), rows)]
    rotation = jax.random.randint(jax.random.fold_in(own, 2), (rows, 1), 0, top)
    return jnp.take_along_axis(table, (jnp.arange(top)[None, :] + rotation) % top, axis=1)


def load_shares(amount, total, most, skew, full):
    loads = [(1 << 20) // math.isqrt(standing ** skew) + 1 for standing in range(1, amount + 1)]
    largest = most if full else min(most, max(-(-total // amount), total * loads[0] // sum(loads)))
    least = 1 if total - largest >= amount - 1 else 0
    given, spare = [largest] + [least] * (amount - 1), total - largest - least * (amount - 1)
    while spare > 0:
        free = [i for i in range(1, amount) if given[i] < largest] or [i for i in range(1, amount) if given[i] < most]
        whole, remaining = sum([loads[i] for i in free]), spare
        for i in free:
            extra = min(most - given[i], max(1, remaining * loads[i] // whole), spare)
            given[i] = given[i] + extra
            spare = spare - extra
    return np.array(given)


def normal_values(key, shape, scale, reach, pieces=(), kind=jnp.bfloat16):
    array = jax.random.normal(key, shape, jnp.float32) * scale
    if len(pieces) > 0:
        array = levels(key, shape, pieces, -0.22, 0.18) * array
    return jnp.clip(array, min=-reach, max=reach).astype(kind)


def setup_inputs(seed: int = 0) -> dict:
    arg_keys = jax.random.split(jax.random.key(seed), 15)
    query_rows = normal_values(arg_keys[0], (TOKENS, QHEADS * HEADDIM), 1.0, 6.0, ((0, 8), (1, 4)))
    key_rows = normal_values(arg_keys[1], (TOKENS, KVHEADS * HEADDIM), 1.0, 6.0, ((0, 8), (1, 4)))
    value_rows = normal_values(arg_keys[2], (TOKENS, KVHEADS * HEADDIM), 1.0, 6.0, ((0, 8), (1, 4)))
    query_gain = draw_query_gain(jax.random.fold_in(arg_keys[14], 71), 0)
    key_gain = jnp.clip(1.0 + 0.18 * jax.random.normal(arg_keys[4], (KVHEADS, HEADDIM), jnp.float32), 0.1, 1.9)
    sink_logits = jnp.clip(1.0 + 5.0 * jax.random.uniform(arg_keys[5], (QHEADS,), jnp.float32) ** levels(arg_keys[5], (QHEADS,), ((0, 4),), -0.2, 0.2), 1.0, 6.0)
    out_weight = normal_values(arg_keys[6], (QHEADS * HEADDIM, WIDTH), (QHEADS * HEADDIM) ** -0.5, 0.109375, ((0, 4),))
    expert_input = normal_values(arg_keys[7], (TOKENS, WIDTH), 1.0, 6.0, ((0, 32),))
    expert_gain = jnp.clip(1.0 + 0.18 * jax.random.normal(arg_keys[8], (WIDTH,), jnp.float32), 0.1, 1.9)
    routes_keys = jax.random.split(jax.random.fold_in(arg_keys[9], 1), TOKENS // ROWS_DEV)
    routes_turns = jax.random.permutation(jax.random.fold_in(arg_keys[9], 3), TOKENS // ROWS_DEV)
    routes = jax.vmap(lambda own, number: assign_block(jax.random.fold_in(arg_keys[9], 2), own, number, ROWS_DEV, EXPERTS, TOPK, CAP, 1))(routes_keys, routes_turns).reshape((TOKENS, TOPK))
    route_logits = normal_values(arg_keys[10], (TOKENS, TOPK), 1.0, 6.0, ((0, 32),), jnp.float32)
    gate_weight = normal_values(arg_keys[11], (EXPERTS, WIDTH, FFN), (WIDTH // 9) ** -0.5, 0.375, ((0, 8), (2, 4)))
    up_weight = normal_values(arg_keys[12], (EXPERTS, WIDTH, FFN), (WIDTH // 9) ** -0.5, 0.375, ((0, 8), (2, 4)))
    down_weight = normal_values(arg_keys[13], (EXPERTS, FFN, WIDTH), (45 * FFN) ** -0.5, 0.01953125, ((0, 8), (1, 4)))
    return dict(query_rows=query_rows, key_rows=key_rows, value_rows=value_rows, query_gain=query_gain, key_gain=key_gain, sink_logits=sink_logits, out_weight=out_weight, expert_input=expert_input, expert_gain=expert_gain, routes=routes, route_logits=route_logits, gate_weight=gate_weight, up_weight=up_weight, down_weight=down_weight)


EPSILON = 1e-06
CLAMP_LIMIT = 7.0
ACT_SLOPE = 1.702
NEGATIVE = -1e+30

def head_norm(row_data, gain_table):
    head_count, head_size = gain_table.shape
    widened = row_data.astype(jnp.float32).reshape(row_data.shape[0], head_count, head_size)
    scaled = widened * lax.rsqrt(lax.optimization_barrier(jnp.mean(widened * widened, axis=-1, keepdims=True)) + EPSILON)
    return (scaled * gain_table).astype(jnp.bfloat16)

def band(padded, blocks):
    tiled = padded.reshape((blocks + 1, WINDOW) + padded.shape[1:])
    return jnp.concatenate([tiled[:-1], tiled[1:]], axis=1)

def blockwise_product(left, right):
    row_total = left.shape[0]
    inner_width = left.shape[1] // N_TP
    left_parts = jnp.transpose(left.reshape(row_total, N_TP, inner_width), (1, 0, 2))
    right_parts = right.reshape(N_TP, inner_width, right.shape[1])

    def accumulate(running, operands):
        left_part, right_part = operands
        partial_value = jnp.dot(left_part, right_part, preferred_element_type=jnp.float32).astype(jnp.bfloat16)
        partial_value = lax.optimization_barrier(partial_value)
        return (running + partial_value.astype(jnp.float32), None)
    running, unused = lax.scan(accumulate, jnp.zeros((row_total, right.shape[1]), jnp.float32), (left_parts, right_parts))
    return running.astype(jnp.bfloat16)

def attention(query_rows, key_rows, value_rows, query_gain, key_gain, sink_logits):
    seq_rows = query_rows.shape[0]
    blocks = seq_rows // WINDOW
    group_size = QHEADS // KVHEADS
    query_hat = head_norm(query_rows, query_gain).reshape(blocks, WINDOW, KVHEADS, group_size, HEADDIM)
    key_hat = head_norm(key_rows, key_gain)
    value_hat = value_rows.reshape(seq_rows, KVHEADS, HEADDIM)
    leading = jnp.zeros((WINDOW, KVHEADS, HEADDIM), jnp.bfloat16)
    key_band = band(jnp.concatenate([leading, key_hat], axis=0), blocks)
    value_band = band(jnp.concatenate([leading, value_hat], axis=0), blocks)
    query_pos = jnp.arange(WINDOW, dtype=jnp.int32)[:, None]
    key_pos = jnp.arange(2 * WINDOW, dtype=jnp.int32)[None, :]
    distance = query_pos + WINDOW - key_pos
    inside = (distance >= 0) & (distance < WINDOW)
    first_block = (jnp.arange(blocks, dtype=jnp.int32) == 0)[:, None, None]
    allowed = inside[None] & ~(first_block & (key_pos < WINDOW)[None])

    def one_head(operands):
        query_part, key_part, value_part, sink_part = operands
        scores = jnp.einsum('bqgd,bjd->bgqj', query_part.astype(jnp.float32), key_part.astype(jnp.float32), precision=lax.Precision.HIGHEST) * HEADDIM ** (-0.5)
        scores = jnp.where(allowed[:, None], scores, NEGATIVE)
        sink_table = sink_part.reshape(1, group_size, 1, 1)
        highest = jnp.maximum(lax.optimization_barrier(jnp.max(scores, axis=-1, keepdims=True)), sink_table)
        weights = jnp.exp(scores - highest)
        total = lax.optimization_barrier(jnp.sum(weights, axis=-1, keepdims=True)) + jnp.exp(sink_table - highest)
        rounded = lax.optimization_barrier(weights.astype(jnp.bfloat16))
        mixed = jnp.einsum('bgqj,bjd->bgqd', rounded.astype(jnp.float32), value_part.astype(jnp.float32), precision=lax.Precision.HIGHEST)
        return (mixed / total).astype(jnp.bfloat16)
    heads_out = lax.map(one_head, (jnp.transpose(query_hat, (2, 0, 1, 3, 4)), jnp.transpose(key_band, (2, 0, 1, 3)), jnp.transpose(value_band, (2, 0, 1, 3)), sink_logits.reshape(KVHEADS, group_size)))
    return jnp.transpose(heads_out, (1, 3, 0, 2, 4)).reshape(seq_rows, QHEADS * HEADDIM)

def slot_maps(route_block):
    flat_routes = route_block.reshape(-1).astype(jnp.int32)
    expert_hot = (flat_routes[:, None] == jnp.arange(EXPERTS, dtype=jnp.int32)[None, :]).astype(jnp.int32)
    before = jnp.cumsum(expert_hot, axis=0) - expert_hot
    return (flat_routes, lax.optimization_barrier(jnp.sum(before * expert_hot, axis=1)).astype(jnp.int32))

def experts_part(expert_input, expert_gain, routes, route_logits, gate_weight, up_weight, down_weight):
    token_count = expert_input.shape[0]
    block_count = token_count // ROWS_DEV
    widened = expert_input.astype(jnp.float32)
    normed = (widened * lax.rsqrt(lax.optimization_barrier(jnp.mean(widened * widened, axis=-1, keepdims=True)) + EPSILON) * expert_gain).astype(jnp.bfloat16)
    route_weight = jax.nn.softmax(route_logits, axis=-1)
    flat_routes, position = jax.vmap(slot_maps)(routes.reshape(block_count, ROWS_DEV, TOPK))
    row_index = jnp.repeat(jnp.arange(ROWS_DEV, dtype=jnp.int32), TOPK)
    block_index = jnp.arange(block_count, dtype=jnp.int32)[:, None]
    sources = jnp.broadcast_to(row_index[None], flat_routes.shape) + block_index * ROWS_DEV
    table = jnp.full((block_count, EXPERTS, CAP), -1, jnp.int32).at[block_index, flat_routes, position].set(sources)
    tables = jnp.transpose(table, (1, 0, 2)).reshape(EXPERTS, block_count * CAP)

    def one_expert(operands):
        slot_index, gate_part, up_part, down_part = operands
        picked = jnp.where((slot_index >= 0)[:, None], normed[jnp.maximum(slot_index, 0).astype(jnp.int32)], jnp.zeros((), jnp.bfloat16))
        gate_pre = jnp.dot(picked, gate_part, preferred_element_type=jnp.float32)
        up_pre = jnp.dot(picked, up_part, preferred_element_type=jnp.float32)
        clipped = jnp.minimum(gate_pre, CLAMP_LIMIT)
        linear = jnp.clip(up_pre, -CLAMP_LIMIT, CLAMP_LIMIT)
        hidden_units = (clipped * jax.nn.sigmoid(ACT_SLOPE * clipped) * (linear + 1.0)).astype(jnp.bfloat16)
        return blockwise_product(hidden_units, down_part)
    outputs = lax.map(one_expert, (tables, gate_weight, up_weight, down_weight))
    slot_place = (block_index * CAP + position).astype(jnp.int32)
    gathered = outputs[flat_routes, slot_place]
    weighted = gathered.astype(jnp.float32).reshape(block_count, ROWS_DEV, TOPK, WIDTH) * route_weight.reshape(block_count, ROWS_DEV, TOPK, 1)
    return lax.optimization_barrier(jnp.sum(weighted, axis=2)).reshape(token_count, WIDTH).astype(jnp.bfloat16)

def reference(query_rows, key_rows, value_rows, query_gain, key_gain, sink_logits, out_weight, expert_input, expert_gain, routes, route_logits, gate_weight, up_weight, down_weight):
    heads_out = attention(query_rows, key_rows, value_rows, query_gain, key_gain, sink_logits)
    attended = blockwise_product(heads_out, out_weight)
    expert_mix = experts_part(expert_input, expert_gain, routes, route_logits, gate_weight, up_weight, down_weight)
    return (attended, expert_mix)
```

```python
import jax
import jax.numpy as jnp
import numpy as np
from jax import lax
from jax.experimental import pallas as pl
from jax.experimental.pallas import tpu as pltpu
from jax.sharding import PartitionSpec as P

EXPERTS = 32
WINDOW = 128


EPSILON = 1e-06
CLAMP_LIMIT = 7.0
ACT_SLOPE = 1.702
NEGATIVE = -1e30


def shifted(value, axis, steps):
    count = lax.axis_size(axis)
    initial, last = (max(0, -steps), min(count, count - steps))
    return lax.ppermute(value, axis, [(source, source + steps) for source in range(initial, last)])


def head_norm(row_data, gain_table):
    head_count, head_size = gain_table.shape
    widened = row_data.astype(jnp.float32).reshape(row_data.shape[0], head_count, head_size)
    scaled = widened * lax.rsqrt(jnp.mean(widened * widened, axis=-1, keepdims=True) + EPSILON)
    return (scaled * gain_table).astype(jnp.bfloat16)


def band(padded, blocks):
    tiled = padded.reshape((blocks + 1, WINDOW) + padded.shape[1:])
    return jnp.concatenate([tiled[:-1], tiled[1:]], axis=1)


def attend(query_rows, key_rows, value_rows, query_gain, key_gain, sink_logits):
    seq_rows = query_rows.shape[0]
    key_heads, head_size = key_gain.shape
    group_size = query_gain.shape[0] // key_heads
    blocks = seq_rows // WINDOW
    query_hat = head_norm(query_rows, query_gain).reshape(
        blocks, WINDOW, key_heads, group_size, head_size
    )
    key_hat = head_norm(key_rows, key_gain)
    value_hat = value_rows.reshape(seq_rows, key_heads, head_size)
    tail_rows = jnp.stack([key_hat[seq_rows - WINDOW :], value_hat[seq_rows - WINDOW :]])
    earlier = shifted(tail_rows, "ep", 1)
    key_band = band(jnp.concatenate([earlier[0], key_hat], axis=0), blocks)
    value_band = band(jnp.concatenate([earlier[1], value_hat], axis=0), blocks)
    query_pos = lax.broadcasted_iota(jnp.int32, (WINDOW, 2 * WINDOW), 0)
    key_pos = lax.broadcasted_iota(jnp.int32, (WINDOW, 2 * WINDOW), 1)
    distance = query_pos + WINDOW - key_pos
    inside = (distance >= 0) & (distance < WINDOW)
    first_block = (lax.broadcasted_iota(jnp.int32, (blocks, 1, 1), 0) == 0) & (
        lax.axis_index("ep") == 0
    )
    allowed = inside[None] & ~(first_block & (key_pos < WINDOW)[None])
    scores = jnp.einsum(
        "bqkgd,bjkd->bkgqj", query_hat, key_band, preferred_element_type=jnp.float32
    ) * head_size ** (-0.5)
    scores = jnp.where(allowed[:, None, None], scores, NEGATIVE)
    sink_table = sink_logits.reshape(1, key_heads, group_size, 1, 1)
    highest = jnp.maximum(jnp.max(scores, axis=-1, keepdims=True), sink_table)
    weights = jnp.exp(scores - highest)
    total = jnp.sum(weights, axis=-1, keepdims=True) + jnp.exp(sink_table - highest)
    mixed = jnp.einsum(
        "bkgqj,bjkd->bkgqd",
        weights.astype(jnp.bfloat16),
        value_band,
        preferred_element_type=jnp.float32,
    )
    mixed = (mixed / total).astype(jnp.bfloat16)
    return jnp.transpose(mixed, (0, 3, 1, 2, 4)).reshape(seq_rows, -1)


def slot_maps(route_block, capacity):
    flat_routes = route_block.reshape(-1)
    expert_hot = (flat_routes[:, None] == lax.broadcasted_iota(jnp.int32, (1, EXPERTS), 1)).astype(
        jnp.int32
    )
    before = jnp.cumsum(expert_hot, axis=0) - expert_hot
    position = jnp.sum(before * expert_hot, axis=1)
    place_hot = (position[:, None] == lax.broadcasted_iota(jnp.int32, (1, capacity), 1)).astype(
        jnp.float32
    )
    row_total, fanout = route_block.shape
    return (
        expert_hot.astype(jnp.float32).reshape(row_total, fanout, EXPERTS),
        place_hot.reshape(row_total, fanout, capacity),
    )


def dispatch_matrix(route_block, capacity):
    expert_hot, place_hot = slot_maps(route_block, capacity)
    return jnp.einsum("rke,rkc->ecr", expert_hot, place_hot).astype(jnp.bfloat16)


def combine_matrix(route_block, route_weight, capacity):
    expert_hot, place_hot = slot_maps(route_block, capacity)
    return jnp.einsum(
        "rke,rkc,rk->rec", expert_hot, place_hot, route_weight, precision=lax.Precision.HIGHEST
    )


def expert_hidden(piece, gate_weight, up_weight):
    gate_pre = jnp.einsum("aecd,edf->aecf", piece, gate_weight, preferred_element_type=jnp.float32)
    up_pre = jnp.einsum("aecd,edf->aecf", piece, up_weight, preferred_element_type=jnp.float32)
    clipped = jnp.minimum(gate_pre, CLAMP_LIMIT)
    linear = jnp.clip(up_pre, -CLAMP_LIMIT, CLAMP_LIMIT)
    return (clipped * jax.nn.sigmoid(ACT_SLOPE * clipped) * (linear + 1.0)).astype(jnp.bfloat16)


MESH = pl.DeviceIdType.MESH
BF = jnp.bfloat16
F32 = jnp.float32


def dot(left, right):
    return jnp.dot(left, right, preferred_element_type=F32)


def activation(gate_pre, up_pre):
    clipped = jnp.minimum(gate_pre, CLAMP_LIMIT)
    linear = jnp.clip(up_pre, -CLAMP_LIMIT, CLAMP_LIMIT)
    return (clipped * jax.nn.sigmoid(ACT_SLOPE * clipped) * (linear + 1.0)).astype(BF)


def iota(shape, axis):
    return lax.broadcasted_iota(jnp.int32, shape, axis)


def fused_kernel(
    dims, tok, gain, info, sink, qgain, kgain, perm, unperm,
    q_hbm, k_hbm, v_hbm, wo_hbm, gate_hbm, up_hbm, down_hbm,
    attended, mixed,
    gate_w, up_w, down_w, wo, qbuf, kext, vext, kd, vd, ho,
    slots, nslots, ntok, ninfo, nrm, gath, xbuf, dbuf, sums, ybuf, retn, retx,
    nsend, nrecv, pbuf, abuf, asend, arecv,
    lsem, zs, zr, ns, nr, ys, yr, ds, dr, rds, rdr, rys, ryr, rzs, rzr, ms, mr,
):
    ep, local, cap, rows, width, ffn, own, seq, kv_heads, q_heads, experts = dims
    lot = ep // 2
    group = 4 * cap
    sorted_rows = 4 * rows
    tile = 512
    pairs = q_heads // 2
    me = lax.axis_index("ep")
    tp = lax.axis_index("tp")
    hi, core = tp // 2, tp % 2
    other = 1 - core
    partner = (me, hi * 2 + other)
    across = (me, (1 - hi) * 2 + core)

    def mate(d):
        found, bit = me, 1
        while bit < ep:
            if d & bit:
                found = found + bit - 2 * bit * (me // bit % 2)
            bit *= 2
        return found

    def remote(src, dst, send, recv, device):
        return pltpu.make_async_remote_copy(
            src_ref=src, dst_ref=dst, send_sem=send, recv_sem=recv,
            device_id=device, device_id_type=MESH,
        )

    halo = WINDOW
    k_in = pltpu.make_async_copy(k_hbm, kext.at[pl.ds(halo, seq)], lsem.at[0])
    v_in = pltpu.make_async_copy(v_hbm, vext.at[pl.ds(halo, seq)], lsem.at[1])
    q_in = pltpu.make_async_copy(q_hbm, qbuf, lsem.at[2])
    wo_in = pltpu.make_async_copy(wo_hbm, wo, lsem.at[3])
    weights = [
        pltpu.make_async_copy(gate_hbm, gate_w, lsem.at[4]),
        pltpu.make_async_copy(up_hbm, up_w, lsem.at[5]),
        pltpu.make_async_copy(down_hbm, down_w, lsem.at[6]),
    ]

    info_y = remote(info, ninfo, ms.at[0], mr.at[0], across)
    tok_y = remote(tok, ntok, ms.at[1], mr.at[1], across)
    following = ((me + 1) % ep, tp)
    k_halo = remote(
        k_hbm.at[pl.ds(seq - halo, halo)], kext.at[pl.ds(0, halo)], ms.at[2], mr.at[2], following
    )
    v_halo = remote(
        v_hbm.at[pl.ds(seq - halo, halo)], vext.at[pl.ds(0, halo)], ms.at[3], mr.at[3], following
    )
    att_d = remote(pbuf.at[other], abuf, ms.at[4], mr.at[4], partner)
    pieces = 4
    piece = own // pieces

    def att_y(i):
        at = pl.ds(i * piece, piece)
        return remote(asend.at[at], arecv.at[at], ms.at[6 + i], mr.at[6 + i], across)

    def mix_y(i):
        at = pl.ds(i * (own // 2), own // 2)
        return remote(nsend.at[at], nrecv.at[at], ms.at[10 + i], mr.at[10 + i], across)

    def z_copy(d):
        return remote(slots.at[d], gath.at[d, core, hi], zs.at[d], zr.at[d], (mate(d), tp))

    def n_copy(d):
        return remote(nslots.at[d], gath.at[d, core, 1 - hi], ns.at[d], nr.at[d], (mate(d), tp))

    def y_copy(d):
        block = gath.at[d, core, hi]
        return remote(block, block, ys.at[d - lot], yr.at[d - lot], across)

    def d_copy(d):
        block = gath.at[d, core]
        return remote(block, block, ds.at[d], dr.at[d], partner)

    def rd_copy(d):
        return remote(gath.at[d, other], dbuf.at[d], rds.at[d], rdr.at[d], partner)

    def ry_copy(d):
        return remote(
            sums.at[d, 1 - hi], ybuf.at[d - lot], rys.at[d - lot], ryr.at[d - lot], across
        )

    def rz_copy(d):
        if d < lot:
            return remote(sums.at[d], retn.at[:, d], rzs.at[d], rzr.at[d], (mate(d), tp))
        return remote(sums.at[d, hi], retx.at[d - lot], rzs.at[d], rzr.at[d], (mate(d), tp))

    def placed(table):
        expert_ids = iota((experts, own), 0).astype(F32)
        hot = [(table[k : k + 1] == expert_ids).astype(F32) for k in range(2)]
        earlier = (iota((own, own), 0) < iota((own, own), 1)).astype(BF)
        before = dot((hot[0] + hot[1]).astype(BF), earlier)
        slot = [
            table[k : k + 1] * cap + jnp.sum(before * hot[k], axis=0, keepdims=True)
            for k in range(2)
        ]
        top = jnp.maximum(table[2:3], table[3:4])
        raised = [jnp.exp(table[2 + k : 3 + k] - top) for k in range(2)]
        share = [raised[k] / (raised[0] + raised[1]) for k in range(2)]
        return slot, share

    def wanted(first, last, axis):
        count = (last - first) * rows
        shape = (count, 1) if axis == 0 else (1, count)
        place = iota(shape, axis)
        found = place
        for d in range(first, last):
            inside = (place >= (d - first) * rows) & (place < (d - first + 1) * rows)
            found = found + jnp.where(inside, (mate(d) - (d - first)) * rows, 0)
        return found.astype(F32)

    def picker(slot, first, last):
        target = wanted(first, last, 0)
        return ((slot[0] == target) | (slot[1] == target)).astype(BF)

    def column(row):
        diagonal = iota((own, own), 0) == iota((own, own), 1)
        return jnp.sum(jnp.where(diagonal, row, 0.0), axis=1, keepdims=True)

    def combiner(slot, share, first, last):
        target = wanted(first, last, 1)
        full = jnp.where(column(slot[0]) == target, column(share[0]), 0.0)
        full = full + jnp.where(column(slot[1]) == target, column(share[1]), 0.0)
        high = full.astype(BF)
        return high, (full - high.astype(F32)).astype(BF)

    def normalise(source):
        wide = source[...].astype(F32)
        mean = jnp.mean(wide * wide, axis=-1, keepdims=True)
        nrm[...] = (wide * lax.rsqrt(mean + EPSILON) * gain[...]).astype(BF)

    for copy in (k_in, v_in, q_in, wo_in):
        copy.start()
    barrier = pltpu.get_barrier_semaphore()
    for d in range(1, ep):
        pl.semaphore_signal(barrier, inc=1, device_id=(mate(d), tp), device_id_type=MESH)
    pl.semaphore_signal(barrier, inc=1, device_id=across, device_id_type=MESH)
    pl.semaphore_signal(barrier, inc=1, device_id=partner, device_id_type=MESH)

    own_slot, own_share = placed(info[...])
    normalise(tok)
    own_pick = picker(own_slot, 0, ep)
    for col in range(0, width, tile):
        picked = dot(own_pick, nrm[:, col : col + tile]).astype(BF)
        slots[:, :, col : col + tile] = picked.reshape(ep, rows, tile)
        gath[0, core, hi, :, col : col + tile] = picked[:rows]

    pl.semaphore_wait(barrier, ep + 1)
    info_y.start()
    tok_y.start()

    @pl.when(me < ep - 1)
    def _():
        k_halo.start()
        v_halo.start()

    for d in list(range(lot, ep)) + list(range(1, lot)):
        z_copy(d).start()
    for copy in weights:
        copy.start()

    low_half = iota((1, 128), 1) < 64
    same_head = (iota((128, 128), 0) // 64 == iota((128, 128), 1) // 64).astype(BF)

    def head_scaled(block, gain_row):
        wide = block.astype(F32)
        square = wide * wide
        high = square.astype(BF)
        rest = (square - high.astype(F32)).astype(BF)
        mean = (dot(high, same_head) + dot(rest, same_head)) * (1.0 / 64.0)
        return wide * lax.rsqrt(mean + EPSILON) * gain_row

    def spread(values, target, m, start, count):
        turned = pltpu.roll(values, 64, 1)
        target[2 * m, pl.ds(start, count)] = jnp.where(low_half, values, turned).astype(BF)
        target[2 * m + 1, pl.ds(start, count)] = jnp.where(low_half, turned, values).astype(BF)

    def prepare(start, count):
        for m in range(kv_heads // 2):
            cols = slice(m * 128, (m + 1) * 128)
            keys = head_scaled(kext[pl.ds(start, count), cols], kgain[m : m + 1])
            spread(keys.astype(BF).astype(F32), kd, m, start, count)
            spread(vext[pl.ds(start, count), cols].astype(F32), vd, m, start, count)

    share_heads = q_heads // kv_heads

    def attend_pair(b, m):
        top_row = pl.multiple_of(b * WINDOW, WINDOW)
        tiles = share_heads
        low_key = jnp.where((b == 0) & (me == 0), WINDOW, 0)
        query = iota((WINDOW, 2 * WINDOW), 0)
        key = iota((WINDOW, 2 * WINDOW), 1)
        allowed = (key > query) & (key <= query + WINDOW) & (key >= low_key)
        for j in range(tiles):
            lane = pl.multiple_of((m * tiles + j) * 128, 128)
            scaled = head_scaled(
                qbuf[pl.ds(top_row, WINDOW), pl.ds(lane, 128)], qgain[pl.ds(m * tiles + j, 1)]
            ).astype(BF).astype(F32) * 0.125
            outs = []
            for half in range(2):
                head = 2 * j + half
                kv = 2 * m + head // share_heads
                mask = low_half if half == 0 else jnp.logical_not(low_half)
                query_hat = jnp.where(mask, scaled, 0.0).astype(BF)
                keys = kd[kv, pl.ds(top_row, 2 * WINDOW)]
                scores = lax.dot_general(
                    query_hat, keys, (((1,), (1,)), ((), ())), preferred_element_type=F32
                )
                scores = jnp.where(allowed, scores, NEGATIVE)
                sink_value = sink[0, 2 * tiles * m + head]
                highest = jnp.maximum(jnp.max(scores, axis=-1, keepdims=True), sink_value)
                raised = jnp.exp(scores - highest)
                total = jnp.sum(raised, axis=-1, keepdims=True) + jnp.exp(sink_value - highest)
                product = dot(raised.astype(BF), vd[kv, pl.ds(top_row, 2 * WINDOW)])
                outs.append(product / total)
            ho[pl.ds(top_row, WINDOW), pl.ds(lane, 128)] = jnp.where(
                low_half, outs[0], outs[1]
            ).astype(BF)

    k_in.wait()
    v_in.wait()

    @pl.when(me == 0)
    def _():
        kext[0:halo] = jnp.zeros((halo, kext.shape[1]), BF)
        vext[0:halo] = jnp.zeros((halo, vext.shape[1]), BF)

    prepare(halo, seq)
    q_in.wait()
    blocks = seq // WINDOW

    def attend_block(i, carry):
        b = (i + 1) % blocks

        @pl.when(i == blocks - 1)
        def _():
            @pl.when(me > 0)
            def _():
                k_halo.wait_recv()
                v_halo.wait_recv()

            prepare(0, halo)

        lax.fori_loop(0, kv_heads // 2, lambda m, c: (attend_pair(b, m), c)[1], 0)
        return carry

    def forward(d):
        z_copy(d).wait_recv()
        y_copy(d).start()

    lax.fori_loop(0, blocks, attend_block, 0)
    forward(lot)
    wo_in.wait()

    def project(i, carry):
        lane = pl.ds(pl.multiple_of(i * 256, 256), 256)
        result = dot(ho[...], wo[:, lane]).astype(BF)
        for t in range(4):
            pbuf[t % 2, t // 2, :, lane] = result[t * own : (t + 1) * own]
        return carry

    lax.fori_loop(0, width // 256, project, 0)
    att_d.start()

    info_y.wait_recv()
    tok_y.wait_recv()
    next_slot, next_share = placed(ninfo[...])
    normalise(ntok)
    next_pick = picker(next_slot, 0, lot)
    for col in range(0, width, tile):
        picked = dot(next_pick, nrm[:, col : col + tile]).astype(BF)
        nslots[:, :, col : col + tile] = picked.reshape(lot, rows, tile)
        gath[0, core, 1 - hi, :, col : col + tile] = picked[:rows]
    for d in range(1, lot):
        n_copy(d).start()
    d_copy(0).start()

    att_d.wait_recv()
    asend[...] = (pbuf[core, 1 - hi].astype(F32) + abuf[1 - hi].astype(F32)).astype(BF)

    def arrange(d, at):
        d_copy(d).wait_recv()
        for col in range(0, width, tile):
            block = gath[d, :, :, :, col : col + tile].reshape(sorted_rows, tile)
            moved = dot(perm[...], block).astype(BF)
            for e in range(local):
                xbuf[e, at : at + group, col : col + tile] = moved[e * group : (e + 1) * group]

    def run(count):
        def expert(e, carry):
            x = xbuf[e, 0:count]
            hidden = activation(dot(x, gate_w[e]), dot(x, up_w[e]))
            for col in range(0, width, tile):
                xbuf[e, 0:count, col : col + tile] = dot(
                    hidden, down_w[e, :, col : col + tile]
                ).astype(BF)
            return carry

        lax.fori_loop(0, local, expert, 0)

    def split(d, at):
        d_copy(d).wait_send()
        if d >= lot:
            y_copy(d).wait_send()
        for col in range(0, width, tile):
            block = jnp.concatenate(
                [xbuf[e, at : at + group, col : col + tile] for e in range(local)], axis=0
            )
            back = dot(unperm[...], block).astype(BF)
            gath[d, :, :, :, col : col + tile] = back.reshape(2, 2, rows, tile)
        rd_copy(d).start()

    def join(d):
        rd_copy(d).wait_recv()
        if d >= lot:
            part = gath[d, core, 1 - hi].astype(F32) + dbuf[d, 1 - hi].astype(F32)
            sums[d, 1 - hi] = part.astype(BF)
            ry_copy(d).start()
            return
        for h in range(2):
            part = (gath[d, core, h].astype(F32) + dbuf[d, h].astype(F32)).astype(BF)
            if d == 0:
                retn[h, 0] = part
            else:
                sums[d, h] = part
        if d > 0:
            rz_copy(d).start()

    def finish(d):
        ry_copy(d).wait_recv()
        total = gath[d, core, hi].astype(F32) + dbuf[d, hi].astype(F32)
        sums[d, hi] = (total + ybuf[d - lot].astype(F32)).astype(BF)
        rz_copy(d).start()

    def hand_over(d):
        if d >= lot:
            y_copy(d).wait_recv()
        elif d > 0:
            z_copy(d).wait_recv()
            n_copy(d).wait_recv()
        if d > 0:
            d_copy(d).start()

    def crossing(d):
        arrange(d, 0)
        run(group)
        split(d, 0)

    forward(lot + 1)
    for copy in weights:
        copy.wait()
    hand_over(lot)
    crossing(lot)
    forward(lot + 2)
    join(lot)
    hand_over(lot + 1)
    att_y(0).start()
    for d in range(1, lot):
        hand_over(d)
    crossing(lot + 1)
    for d in range(lot):
        arrange(d, d * group)
    finish(lot)
    join(lot + 1)
    run(lot * group)
    forward(lot + 3)
    for d in range(1, lot):
        split(d, d * group)
        if d > 1:
            join(d - 1)
    split(0, 0)
    join(lot - 1)
    join(0)
    hand_over(lot + 2)
    finish(lot + 1)
    crossing(lot + 2)
    att_y(1).start()
    hand_over(lot + 3)
    join(lot + 2)
    crossing(lot + 3)
    finish(lot + 2)
    join(lot + 3)
    att_y(2).start()
    att_y(3).start()
    next_near = combiner(next_slot, next_share, 0, lot)
    for d in range(1, lot):
        rz_copy(d).wait_recv()
    for col in range(0, width, tile):
        near = retn[1 - hi, :, :, col : col + tile].reshape(lot * rows, tile)
        total = dot(next_near[0], near) + dot(next_near[1], near)
        nsend[:, col : col + tile] = total.astype(BF)
    for i in range(2):
        mix_y(i).start()
    finish(lot + 3)

    own_near = combiner(own_slot, own_share, 0, lot)
    own_far = combiner(own_slot, own_share, lot, ep)
    for d in range(lot, ep):
        rz_copy(d).wait_recv()
    for i in range(2):
        mix_y(i).wait_recv()
    for col in range(0, width, tile):
        near = retn[hi, :, :, col : col + tile].reshape(lot * rows, tile)
        far = retx[:, :, col : col + tile].reshape(lot * rows, tile)
        total = dot(own_near[0], near) + dot(own_near[1], near)
        total = total + dot(own_far[0], far) + dot(own_far[1], far)
        total = total + nrecv[:, col : col + tile].astype(F32)
        mixed[:, col : col + tile] = total.astype(BF)
    for i in range(pieces):
        att_y(i).wait_recv()
    whole = pbuf[core, hi].astype(F32) + abuf[hi].astype(F32) + arecv[...].astype(F32)
    attended[...] = whole.astype(BF)

    @pl.when(me < ep - 1)
    def _():
        k_halo.wait_send()
        v_halo.wait_send()

    for copy in [info_y, tok_y, att_d, mix_y(0), mix_y(1)] + [att_y(i) for i in range(pieces)]:
        copy.wait_send()
    for d in range(ep):
        rd_copy(d).wait_send()
        if d > 0:
            z_copy(d).wait_send()
            rz_copy(d).wait_send()
        if 0 < d < lot:
            n_copy(d).wait_send()
        if d >= lot:
            ry_copy(d).wait_send()


def run_fused(dims, tok, gain, info, sink, qgain, kgain, streams):
    ep, local, cap, rows, width, ffn, own, seq, kv_heads, q_heads, experts = dims
    lot = ep // 2
    order = np.arange(local * 4 * cap)
    e, t, c = order // (4 * cap), order // cap % 4, order % cap
    perm = (t * rows + e * cap + c)[:, None] == np.arange(4 * rows)[None, :]
    perm = jnp.asarray(perm, BF)
    dma = pltpu.SemaphoreType.DMA
    vm = pl.BlockSpec(memory_space=pltpu.VMEM)
    anys = pl.BlockSpec(memory_space=pl.ANY)
    kv_width = kv_heads * 64

    def held(*shape, dtype=BF):
        return pltpu.VMEM(shape, dtype)

    return pl.pallas_call(
        lambda *refs: fused_kernel(dims, *refs),
        name="fused_layer",
        out_shape=(
            jax.ShapeDtypeStruct((own, width), BF), jax.ShapeDtypeStruct((own, width), BF)
        ),
        in_specs=[vm, vm, vm, pl.BlockSpec(memory_space=pltpu.SMEM)] + [vm] * 4 + [anys] * 7,
        out_specs=(vm, vm),
        scratch_shapes=[
            held(local, width, ffn), held(local, width, ffn), held(local, ffn, width),
            held(q_heads * 64, width),
            held(seq, q_heads * 64),
            held(seq + WINDOW, kv_width), held(seq + WINDOW, kv_width),
            held(kv_heads, seq + WINDOW, 128), held(kv_heads, seq + WINDOW, 128),
            held(seq, q_heads * 64),
            held(ep, rows, width), held(lot, rows, width),
            held(own, width), held(8, own, dtype=F32), held(own, width),
            held(ep, 2, 2, rows, width),
            held(local, lot * 4 * cap, width),
            held(ep, 2, rows, width), held(ep, 2, rows, width),
            held(lot, rows, width),
            held(2, lot, rows, width), held(lot, rows, width),
            held(own, width), held(own, width),
            held(2, 2, own, width), held(2, own, width), held(own, width), held(own, width),
            dma((7,)),
            dma((ep,)), dma((ep,)),
            dma((lot,)), dma((lot,)),
            dma((lot,)), dma((lot,)),
            dma((ep,)), dma((ep,)),
            dma((ep,)), dma((ep,)),
            dma((lot,)), dma((lot,)),
            dma((ep,)), dma((ep,)),
            dma((12,)), dma((12,)),
        ],
        compiler_params=pltpu.CompilerParams(
            collective_id=0, has_side_effects=True, vmem_limit_bytes=67043328
        ),
    )(tok, gain, info, sink, qgain, kgain, perm, perm.T, *streams)


def fits(dims, tp, kv_size):
    ep, local, cap, rows, width, ffn, own, seq, kv_heads, q_heads, experts = dims
    if tp != 4 or ep < 4 or ep & (ep - 1) or rows % 16 or cap % 4 or kv_size != 64:
        return False
    if own != 128 or seq != 4 * own or kv_heads % 2 or q_heads != 3 * kv_heads or width % 512:
        return False
    lot = ep // 2
    held = 3 * local * width * ffn + q_heads * 64 * width + 3 * seq * q_heads * 64
    held += rows * width * (11 * ep + 5 * lot) + local * lot * 4 * cap * width + 14 * own * width
    return 2 * held < 63 * 1024 * 1024


def on_device(
    query_rows,
    key_rows,
    value_rows,
    query_gain,
    key_gain,
    sink_logits,
    out_weight,
    expert_input,
    expert_gain,
    routes,
    route_logits,
    gate_weight,
    up_weight,
    down_weight,
):
    own_rows = expert_input.shape[0]
    fanout = routes.shape[1]
    capacity = (3 * own_rows * fanout + 2 * EXPERTS - 1) // (2 * EXPERTS)
    ep_size = lax.axis_size("ep")
    tp_size = lax.axis_size("tp")
    local_experts = gate_weight.shape[0]
    key_heads, head_size = key_gain.shape
    dims = (
        ep_size, local_experts, capacity, local_experts * capacity, expert_input.shape[1],
        gate_weight.shape[2], own_rows, query_rows.shape[0], key_heads, query_gain.shape[0],
        EXPERTS,
    )
    if fits(dims, tp_size, head_size):
        info = jnp.concatenate(
            [routes.astype(F32), route_logits, jnp.zeros((own_rows, 4), F32)], axis=1
        ).T
        return run_fused(
            dims, expert_input, expert_gain.reshape(1, -1), info, sink_logits.reshape(1, -1),
            query_gain.reshape(-1, 2 * head_size), key_gain.reshape(-1, 2 * head_size),
            (query_rows, key_rows, value_rows, out_weight, gate_weight, up_weight, down_weight),
        )
    heads_out = attend(query_rows, key_rows, value_rows, query_gain, key_gain, sink_logits)
    projected = jnp.dot(heads_out, out_weight, preferred_element_type=jnp.float32).astype(
        jnp.bfloat16
    )
    widened = expert_input.astype(jnp.float32)
    normed = (
        widened
        * lax.rsqrt(jnp.mean(widened * widened, axis=-1, keepdims=True) + EPSILON)
        * expert_gain
    ).astype(jnp.bfloat16)
    route_weight = jax.nn.softmax(route_logits, axis=-1)
    attended = lax.psum_scatter(projected, "tp", scatter_dimension=0, tiled=True)
    combine = combine_matrix(routes, route_weight, capacity)
    sender = dispatch_matrix(routes, capacity)
    slot_rows = jnp.einsum(
        "ecr,rd->ecd", sender, normed, preferred_element_type=jnp.float32
    ).astype(jnp.bfloat16)
    slot_rows = slot_rows.reshape(ep_size, local_experts, capacity, -1)
    arrived = lax.all_to_all(slot_rows, "ep", split_axis=0, concat_axis=0, tiled=True)
    hidden_units = expert_hidden(
        lax.all_gather(arrived, "tp", axis=0, tiled=True), gate_weight, up_weight
    )
    partial_value = jnp.einsum(
        "aecf,efd->aecd", hidden_units, down_weight, preferred_element_type=jnp.float32
    ).astype(jnp.bfloat16)
    partial_value = partial_value.reshape(tp_size, ep_size * local_experts * capacity, -1)
    pieces = lax.all_to_all(partial_value, "tp", split_axis=0, concat_axis=0, tiled=True)
    summed = jnp.sum(pieces, axis=0, dtype=jnp.float32).astype(jnp.bfloat16)
    summed = summed.reshape(ep_size, local_experts * capacity, -1)
    returned = lax.all_to_all(summed, "ep", split_axis=0, concat_axis=0, tiled=True).reshape(
        EXPERTS, capacity, -1
    )
    expert_mix = jnp.einsum(
        "rec,ecd->rd", combine, returned.astype(jnp.float32), precision=lax.Precision.HIGHEST
    ).astype(jnp.bfloat16)
    return (attended, expert_mix)


def solution(mesh):
    placed = (
        P("ep", "tp"),
        P("ep", "tp"),
        P("ep", "tp"),
        P("tp", None),
        P("tp", None),
        P("tp"),
        P("tp", None),
        P(("ep", "tp"), None),
        P(),
        P(("ep", "tp"), None),
        P(("ep", "tp"), None),
        P("ep", None, "tp"),
        P("ep", None, "tp"),
        P("ep", "tp", None),
    )
    return jax.shard_map(
        on_device,
        mesh=mesh,
        in_specs=placed,
        out_specs=(P(("ep", "tp"), None), P(("ep", "tp"), None)),
        check_vma=False,
    )
```

```python
import jax
import jax.numpy as jnp
import numpy as np
from jax import lax
from jax.experimental import pallas as pl
from jax.experimental.pallas import tpu as pltpu
from jax.sharding import PartitionSpec as P

EXPERTS = 32
WINDOW = 128


EPSILON = 1e-06
CLAMP_LIMIT = 7.0
ACT_SLOPE = 1.702
NEGATIVE = -1e30


def shifted(value, axis, steps):
    count = lax.axis_size(axis)
    initial, last = (max(0, -steps), min(count, count - steps))
    return lax.ppermute(value, axis, [(source, source + steps) for source in range(initial, last)])


def head_norm(row_data, gain_table):
    head_count, head_size = gain_table.shape
    widened = row_data.astype(jnp.float32).reshape(row_data.shape[0], head_count, head_size)
    scaled = widened * lax.rsqrt(jnp.mean(widened * widened, axis=-1, keepdims=True) + EPSILON)
    return (scaled * gain_table).astype(jnp.bfloat16)


def band(padded, blocks):
    tiled = padded.reshape((blocks + 1, WINDOW) + padded.shape[1:])
    return jnp.concatenate([tiled[:-1], tiled[1:]], axis=1)


def attend(query_rows, key_rows, value_rows, query_gain, key_gain, sink_logits):
    seq_rows = query_rows.shape[0]
    key_heads, head_size = key_gain.shape
    group_size = query_gain.shape[0] // key_heads
    blocks = seq_rows // WINDOW
    query_hat = head_norm(query_rows, query_gain).reshape(
        blocks, WINDOW, key_heads, group_size, head_size
    )
    key_hat = head_norm(key_rows, key_gain)
    value_hat = value_rows.reshape(seq_rows, key_heads, head_size)
    tail_rows = jnp.stack([key_hat[seq_rows - WINDOW :], value_hat[seq_rows - WINDOW :]])
    earlier = shifted(tail_rows, "ep", 1)
    key_band = band(jnp.concatenate([earlier[0], key_hat], axis=0), blocks)
    value_band = band(jnp.concatenate([earlier[1], value_hat], axis=0), blocks)
    query_pos = lax.broadcasted_iota(jnp.int32, (WINDOW, 2 * WINDOW), 0)
    key_pos = lax.broadcasted_iota(jnp.int32, (WINDOW, 2 * WINDOW), 1)
    distance = query_pos + WINDOW - key_pos
    inside = (distance >= 0) & (distance < WINDOW)
    first_block = (lax.broadcasted_iota(jnp.int32, (blocks, 1, 1), 0) == 0) & (
        lax.axis_index("ep") == 0
    )
    allowed = inside[None] & ~(first_block & (key_pos < WINDOW)[None])
    scores = jnp.einsum(
        "bqkgd,bjkd->bkgqj", query_hat, key_band, preferred_element_type=jnp.float32
    ) * head_size ** (-0.5)
    scores = jnp.where(allowed[:, None, None], scores, NEGATIVE)
    sink_table = sink_logits.reshape(1, key_heads, group_size, 1, 1)
    highest = jnp.maximum(jnp.max(scores, axis=-1, keepdims=True), sink_table)
    weights = jnp.exp(scores - highest)
    total = jnp.sum(weights, axis=-1, keepdims=True) + jnp.exp(sink_table - highest)
    mixed = jnp.einsum(
        "bkgqj,bjkd->bkgqd",
        weights.astype(jnp.bfloat16),
        value_band,
        preferred_element_type=jnp.float32,
    )
    mixed = (mixed / total).astype(jnp.bfloat16)
    return jnp.transpose(mixed, (0, 3, 1, 2, 4)).reshape(seq_rows, -1)


def slot_maps(route_block, capacity):
    flat_routes = route_block.reshape(-1)
    expert_hot = (flat_routes[:, None] == lax.broadcasted_iota(jnp.int32, (1, EXPERTS), 1)).astype(
        jnp.int32
    )
    before = jnp.cumsum(expert_hot, axis=0) - expert_hot
    position = jnp.sum(before * expert_hot, axis=1)
    place_hot = (position[:, None] == lax.broadcasted_iota(jnp.int32, (1, capacity), 1)).astype(
        jnp.float32
    )
    row_total, fanout = route_block.shape
    return (
        expert_hot.astype(jnp.float32).reshape(row_total, fanout, EXPERTS),
        place_hot.reshape(row_total, fanout, capacity),
    )


def dispatch_matrix(route_block, capacity):
    expert_hot, place_hot = slot_maps(route_block, capacity)
    return jnp.einsum("rke,rkc->ecr", expert_hot, place_hot).astype(jnp.bfloat16)


def combine_matrix(route_block, route_weight, capacity):
    expert_hot, place_hot = slot_maps(route_block, capacity)
    return jnp.einsum(
        "rke,rkc,rk->rec", expert_hot, place_hot, route_weight, precision=lax.Precision.HIGHEST
    )


def expert_hidden(piece, gate_weight, up_weight):
    gate_pre = jnp.einsum("aecd,edf->aecf", piece, gate_weight, preferred_element_type=jnp.float32)
    up_pre = jnp.einsum("aecd,edf->aecf", piece, up_weight, preferred_element_type=jnp.float32)
    clipped = jnp.minimum(gate_pre, CLAMP_LIMIT)
    linear = jnp.clip(up_pre, -CLAMP_LIMIT, CLAMP_LIMIT)
    return (clipped * jax.nn.sigmoid(ACT_SLOPE * clipped) * (linear + 1.0)).astype(jnp.bfloat16)


VMEM_LIMIT = 67043328
MESH = pl.DeviceIdType.MESH
BF = jnp.bfloat16
F32 = jnp.float32


def dot(left, right):
    return jnp.dot(left, right, preferred_element_type=F32)


def activation(gate_pre, up_pre):
    clipped = jnp.minimum(gate_pre, CLAMP_LIMIT)
    linear = jnp.clip(up_pre, -CLAMP_LIMIT, CLAMP_LIMIT)
    return (clipped * jax.nn.sigmoid(ACT_SLOPE * clipped) * (linear + 1.0)).astype(BF)


def iota(shape, axis):
    return lax.broadcasted_iota(jnp.int32, shape, axis)


def fused_kernel(
    dims, tok, gain, routes, logits, sink, qgain, kgain, perm, unperm,
    q_hbm, k_hbm, v_hbm, wo_hbm, gate_hbm, up_hbm, down_hbm,
    attended, mixed,
    qpair, gate_w, up_w, down_w, wo, qbuf, kext, vext, kd, vd, ho,
    slots, nslots, ntok, nroutes, nlogits, nrm, gath, xbuf, dbuf, sums, ybuf, retn, retx,
    nsend, nrecv, pbuf, abuf, asend, arecv,
    lsem, zs, zr, ns, nr, ys, yr, ds, dr, rds, rdr, rys, ryr, rzs, rzr, ms, mr,
):
    ep, local, cap, rows, width, ffn, own, seq, kv_heads, q_heads, experts = dims
    lot = ep // 2
    group = 4 * cap
    sorted_rows = 4 * rows
    tile = 512
    pairs = q_heads // 2
    me = lax.axis_index("ep")
    tp = lax.axis_index("tp")
    hi, core = tp // 2, tp % 2
    other = 1 - core
    partner = (me, hi * 2 + other)
    across = (me, (1 - hi) * 2 + core)

    def mate(d):
        found, bit = 0, 1
        while bit < ep:
            found = found + (me // bit + d // bit) % 2 * bit
            bit *= 2
        return found

    inner = (me // (ep // 4) + 1) // 2 % 2

    def far(i):
        return lot + (i + lot // 2) % lot

    def remote(src, dst, send, recv, device):
        return pltpu.make_async_remote_copy(
            src_ref=src, dst_ref=dst, send_sem=send, recv_sem=recv,
            device_id=device, device_id_type=MESH,
        )

    halo = WINDOW
    k_in = pltpu.make_async_copy(k_hbm, kext.at[pl.ds(halo, seq)], lsem.at[0])
    v_in = pltpu.make_async_copy(v_hbm, vext.at[pl.ds(halo, seq)], lsem.at[1])
    q_in = pltpu.make_async_copy(q_hbm, qbuf, lsem.at[2])
    wo_in = pltpu.make_async_copy(wo_hbm, wo, lsem.at[3])
    weights = [
        pltpu.make_async_copy(gate_hbm, gate_w, lsem.at[4]),
        pltpu.make_async_copy(up_hbm, up_w, lsem.at[5]),
        pltpu.make_async_copy(down_hbm, down_w, lsem.at[6]),
    ]

    routes_y = remote(routes, nroutes, ms.at[0], mr.at[0], across)
    logits_y = remote(logits, nlogits, ms.at[5], mr.at[5], across)
    tok_y = remote(tok, ntok, ms.at[1], mr.at[1], across)
    following = ((me + 1) % ep, tp)
    k_halo = remote(
        k_hbm.at[pl.ds(seq - halo, halo)], kext.at[pl.ds(0, halo)], ms.at[2], mr.at[2], following
    )
    v_halo = remote(
        v_hbm.at[pl.ds(seq - halo, halo)], vext.at[pl.ds(0, halo)], ms.at[3], mr.at[3], following
    )
    att_d = remote(pbuf.at[other], abuf, ms.at[4], mr.at[4], partner)
    pieces = 4
    piece = own // pieces

    def att_y(i):
        at = pl.ds(i * piece, piece)
        return remote(asend.at[at], arecv.at[at], ms.at[6 + i], mr.at[6 + i], across)

    def mix_y(i):
        at = pl.ds(i * (own // 2), own // 2)
        return remote(nsend.at[at], nrecv.at[at], ms.at[10 + i], mr.at[10 + i], across)

    def z_copy(d):
        return remote(slots.at[d], gath.at[d, core, hi], zs.at[d], zr.at[d], (mate(d), tp))

    def n_copy(d):
        return remote(nslots.at[d], gath.at[d, core, 1 - hi], ns.at[d], nr.at[d], (mate(d), tp))

    def y_copy(d):
        block = gath.at[d, core, hi]
        return remote(block, block, ys.at[d - lot], yr.at[d - lot], across)

    def d_copy(d):
        block = gath.at[d, core]
        return remote(block, block, ds.at[d], dr.at[d], partner)

    def rd_copy(d):
        return remote(gath.at[d, other], dbuf.at[d], rds.at[d], rdr.at[d], partner)

    def ry_copy(d):
        return remote(
            sums.at[d, 1 - hi], ybuf.at[d - lot], rys.at[d - lot], ryr.at[d - lot], across
        )

    def near_copy(d):
        return remote(sums.at[d], retn.at[:, d], rzs.at[d], rzr.at[d], (mate(d), tp))

    def rz_copy(d):
        return remote(sums.at[d, hi], retx.at[d - lot], rzs.at[d], rzr.at[d], (mate(d), tp))

    def placed(routed, scores):
        table = routed.astype(F32)
        expert_ids = iota((experts, own), 0).astype(F32)
        hot = [(table[k : k + 1] == expert_ids).astype(F32) for k in range(2)]
        earlier = (iota((own, own), 0) < iota((own, own), 1)).astype(BF)
        before = dot((hot[0] + hot[1]).astype(BF), earlier)
        slot = [
            table[k : k + 1] * cap + jnp.sum(before * hot[k], axis=0, keepdims=True)
            for k in range(2)
        ]
        top = jnp.maximum(scores[0:1], scores[1:2])
        raised = [jnp.exp(scores[k : k + 1] - top) for k in range(2)]
        share = [raised[k] / (raised[0] + raised[1]) for k in range(2)]
        return slot, share

    def wanted(first, last, axis):
        count = (last - first) * rows
        shape = (count, 1) if axis == 0 else (1, count)
        place = iota(shape, axis)
        found = place
        for d in range(first, last):
            inside = (place >= (d - first) * rows) & (place < (d - first + 1) * rows)
            found = found + jnp.where(inside, (mate(d) - (d - first)) * rows, 0)
        return found.astype(F32)

    def picker(slot, first, last):
        target = wanted(first, last, 0)
        return ((slot[0] == target) | (slot[1] == target)).astype(BF)

    def column(row):
        diagonal = iota((own, own), 0) == iota((own, own), 1)
        return jnp.sum(jnp.where(diagonal, row, 0.0), axis=1, keepdims=True)

    def combiner(slot, share, first, last):
        target = wanted(first, last, 1)
        full = jnp.where(column(slot[0]) == target, column(share[0]), 0.0)
        full = full + jnp.where(column(slot[1]) == target, column(share[1]), 0.0)
        high = full.astype(BF)
        return high, (full - high.astype(F32)).astype(BF)

    def normalise(source):
        wide = source[...].astype(F32)
        mean = jnp.mean(wide * wide, axis=-1, keepdims=True)
        nrm[...] = (wide * lax.rsqrt(mean + EPSILON) * gain[...]).astype(BF)

    for copy in (k_in, v_in, q_in, wo_in):
        copy.start()
    barrier = pltpu.get_barrier_semaphore()
    for d in range(1, ep):
        pl.semaphore_signal(barrier, inc=1, device_id=(mate(d), tp), device_id_type=MESH)
    pl.semaphore_signal(barrier, inc=1, device_id=across, device_id_type=MESH)
    pl.semaphore_signal(barrier, inc=1, device_id=partner, device_id_type=MESH)

    own_slot, own_share = placed(routes[...], logits[...])
    normalise(tok)
    own_pick = picker(own_slot, 0, ep)
    for col in range(0, width, tile):
        picked = dot(own_pick, nrm[:, col : col + tile]).astype(BF)
        slots[:, :, col : col + tile] = picked.reshape(ep, rows, tile)
        gath[0, core, hi, :, col : col + tile] = picked[:rows]

    pl.semaphore_wait(barrier, ep + 1)
    routes_y.start()
    logits_y.start()
    tok_y.start()

    @pl.when(me < ep - 1)
    def _():
        k_halo.start()
        v_halo.start()

    for i in range(lot // 2):
        z_copy(far(i)).start()
    for d in range(1, lot):
        z_copy(d).start()
    for copy in weights:
        copy.start()

    low_half = iota((1, 128), 1) < 64
    same_head = (iota((128, 128), 0) // 64 == iota((128, 128), 1) // 64).astype(BF)

    def gain_pair(table, t):
        return jnp.concatenate([table[2 * t : 2 * t + 1], table[2 * t + 1 : 2 * t + 2]], axis=1)

    for t in range(pairs):
        qpair[t : t + 1] = gain_pair(qgain, t)

    def head_scaled(block, gain_row):
        wide = block.astype(F32)
        square = wide * wide
        high = square.astype(BF)
        rest = (square - high.astype(F32)).astype(BF)
        mean = (dot(high, same_head) + dot(rest, same_head)) * (1.0 / 64.0)
        return wide * lax.rsqrt(mean + EPSILON) * gain_row

    def spread(values, target, m, start, count):
        turned = pltpu.roll(values, 64, 1)
        target[2 * m, pl.ds(start, count)] = jnp.where(low_half, values, turned).astype(BF)
        target[2 * m + 1, pl.ds(start, count)] = jnp.where(low_half, turned, values).astype(BF)

    def prepare(start, count):
        for m in range(kv_heads // 2):
            cols = slice(m * 128, (m + 1) * 128)
            keys = head_scaled(kext[pl.ds(start, count), cols], gain_pair(kgain, m))
            spread(keys.astype(BF).astype(F32), kd, m, start, count)
            spread(vext[pl.ds(start, count), cols].astype(F32), vd, m, start, count)

    share_heads = q_heads // kv_heads

    def attend_pair(b, m):
        top_row = pl.multiple_of(b * WINDOW, WINDOW)
        tiles = share_heads
        low_key = jnp.where((b == 0) & (me == 0), WINDOW, 0)
        query = iota((WINDOW, 2 * WINDOW), 0)
        key = iota((WINDOW, 2 * WINDOW), 1)
        allowed = (key > query) & (key <= query + WINDOW) & (key >= low_key)
        for j in range(tiles):
            lane = pl.multiple_of((m * tiles + j) * 128, 128)
            scaled = head_scaled(
                qbuf[pl.ds(top_row, WINDOW), pl.ds(lane, 128)], qpair[pl.ds(m * tiles + j, 1)]
            ).astype(BF).astype(F32) * 0.125
            outs = []
            for half in range(2):
                head = 2 * j + half
                kv = 2 * m + head // share_heads
                mask = low_half if half == 0 else jnp.logical_not(low_half)
                query_hat = jnp.where(mask, scaled, 0.0).astype(BF)
                keys = kd[kv, pl.ds(top_row, 2 * WINDOW)]
                scores = lax.dot_general(
                    query_hat, keys, (((1,), (1,)), ((), ())), preferred_element_type=F32
                )
                scores = jnp.where(allowed, scores, NEGATIVE)
                sink_value = sink[0, 2 * tiles * m + head]
                highest = jnp.maximum(jnp.max(scores, axis=-1, keepdims=True), sink_value)
                raised = jnp.exp(scores - highest)
                total = jnp.sum(raised, axis=-1, keepdims=True) + jnp.exp(sink_value - highest)
                product = dot(raised.astype(BF), vd[kv, pl.ds(top_row, 2 * WINDOW)])
                outs.append(product / total)
            ho[pl.ds(top_row, WINDOW), pl.ds(lane, 128)] = jnp.where(
                low_half, outs[0], outs[1]
            ).astype(BF)

    k_in.wait()
    v_in.wait()

    @pl.when(me == 0)
    def _():
        kext[0:halo] = jnp.zeros((halo, kext.shape[1]), BF)
        vext[0:halo] = jnp.zeros((halo, vext.shape[1]), BF)

    prepare(halo, seq)
    q_in.wait()
    blocks = seq // WINDOW

    def attend_block(i, carry):
        b = (i + 1) % blocks

        @pl.when(i == blocks - 1)
        def _():
            @pl.when(me > 0)
            def _():
                k_halo.wait_recv()
                v_halo.wait_recv()

            prepare(0, halo)

        lax.fori_loop(0, kv_heads // 2, lambda m, c: (attend_pair(b, m), c)[1], 0)

        return carry

    def forward(d):
        z_copy(d).wait_recv()
        y_copy(d).start()

    def at_edge(step):
        pl.when(inner == 0)(step)

    def at_middle(step):
        pl.when(inner == 1)(step)

    lax.fori_loop(0, blocks, attend_block, 0)
    wo_in.wait()

    def project(i, carry):
        lane = pl.ds(pl.multiple_of(i * 256, 256), 256)
        result = dot(ho[...], wo[:, lane]).astype(BF)
        for t in range(4):
            pbuf[t % 2, t // 2, :, lane] = result[t * own : (t + 1) * own]
        return carry

    lax.fori_loop(0, width // 256, project, 0)
    att_d.start()

    forward(far(0))
    routes_y.wait_recv()
    logits_y.wait_recv()
    tok_y.wait_recv()
    next_slot, next_share = placed(nroutes[...], nlogits[...])
    normalise(ntok)
    next_pick = picker(next_slot, 0, lot)
    for col in range(0, width, tile):
        picked = dot(next_pick, nrm[:, col : col + tile]).astype(BF)
        nslots[:, :, col : col + tile] = picked.reshape(lot, rows, tile)
        gath[0, core, 1 - hi, :, col : col + tile] = picked[:rows]
    for d in range(1, lot):
        n_copy(d).start()
    for i in range(lot // 2, lot):
        z_copy(far(i)).start()
    d_copy(0).start()

    forward(far(1))
    att_d.wait_recv()
    asend[...] = (pbuf[core, 1 - hi].astype(F32) + abuf[1 - hi].astype(F32)).astype(BF)
    def arrange(d, at):
        d_copy(d).wait_recv()
        for col in range(0, width, tile):
            block = gath[d, :, :, :, col : col + tile].reshape(sorted_rows, tile)
            moved = dot(perm[...], block).astype(BF)
            for e in range(local):
                xbuf[e, at : at + group, col : col + tile] = moved[e * group : (e + 1) * group]

    def run(at, count, first=0, last=local):
        def expert(e, carry):
            x = xbuf[e, at : at + count]
            hidden = activation(dot(x, gate_w[e]), dot(x, up_w[e]))
            for col in range(0, width, tile):
                xbuf[e, at : at + count, col : col + tile] = dot(
                    hidden, down_w[e, :, col : col + tile]
                ).astype(BF)
            return carry

        lax.fori_loop(first, last, expert, 0)

    def split(d, at, crossed):
        d_copy(d).wait_send()
        if crossed:
            y_copy(d).wait_send()
        for col in range(0, width, tile):
            block = jnp.concatenate(
                [xbuf[e, at : at + group, col : col + tile] for e in range(local)], axis=0
            )
            back = dot(unperm[...], block).astype(BF)
            gath[d, :, :, :, col : col + tile] = back.reshape(2, 2, rows, tile)
        rd_copy(d).start()

    def join(d):
        rd_copy(d).wait_recv()
        part = gath[d, core, 1 - hi].astype(F32) + dbuf[d, 1 - hi].astype(F32)
        sums[d, 1 - hi] = part.astype(BF)
        ry_copy(d).start()

    def near_join(d):
        rd_copy(d).wait_recv()
        for h in range(2):
            part = (gath[d, core, h].astype(F32) + dbuf[d, h].astype(F32)).astype(BF)
            if d == 0:
                retn[h, 0] = part
            else:
                sums[d, h] = part
        if d > 0:
            near_copy(d).start()

    def finish(d):
        ry_copy(d).wait_recv()
        total = gath[d, core, hi].astype(F32) + dbuf[d, hi].astype(F32)
        sums[d, hi] = (total + ybuf[d - lot].astype(F32)).astype(BF)
        rz_copy(d).start()

    def hand_over(d):
        y_copy(d).wait_recv()
        d_copy(d).start()

    def near_hand_over(d):
        z_copy(d).wait_recv()
        n_copy(d).wait_recv()
        d_copy(d).start()

    def near_sum():
        near_pick = combiner(next_slot, next_share, 0, lot)
        for d in range(1, lot):
            near_copy(d).wait_recv()
        for col in range(0, width, tile):
            near = retn[1 - hi, :, :, col : col + tile].reshape(lot * rows, tile)
            total = dot(near_pick[0], near) + dot(near_pick[1], near)
            nsend[:, col : col + tile] = total.astype(BF)
        for i in range(2):
            mix_y(i).start()

    att_y(0).start()
    att_y(1).start()
    for copy in weights:
        copy.wait()
    hand_over(far(0))
    arrange(far(0), 0)
    run(0, group)
    hand_over(far(1))
    split(far(0), 0, True)
    arrange(far(1), 0)
    join(far(0))
    run(0, group)
    for d in range(1, lot):
        near_hand_over(d)
    split(far(1), 0, True)
    forward(far(2))
    arrange(0, 0)
    join(far(1))
    finish(far(0))
    for d in range(1, lot):
        arrange(d, d * group)
    run(0, lot * group, 0, 2)
    forward(far(3))
    att_y(2).start()
    att_y(3).start()
    run(0, lot * group, 2, 4)
    split(1, group, False)
    split(2, 2 * group, False)
    hand_over(far(2))
    near_join(1)
    split(3, 3 * group, False)
    near_join(2)
    split(0, 0, False)
    arrange(far(2), 0)
    near_join(3)
    finish(far(1))
    run(0, group)
    split(far(2), 0, True)
    hand_over(far(3))
    arrange(far(3), group)
    join(far(2))
    run(group, group, 0, 3)
    near_join(0)
    finish(far(2))
    run(group, group, 3, 4)
    split(far(3), group, True)
    join(far(3))
    finish(far(3))
    near_sum()

    own_near = combiner(own_slot, own_share, 0, lot)
    own_far = combiner(own_slot, own_share, lot, ep)
    for d in range(lot, ep):
        rz_copy(d).wait_recv()
    for i in range(2):
        mix_y(i).wait_recv()
    for col in range(0, width, tile):
        near = retn[hi, :, :, col : col + tile].reshape(lot * rows, tile)
        far = retx[:, :, col : col + tile].reshape(lot * rows, tile)
        total = dot(own_near[0], near) + dot(own_near[1], near)
        total = total + dot(own_far[0], far) + dot(own_far[1], far)
        total = total + nrecv[:, col : col + tile].astype(F32)
        mixed[:, col : col + tile] = total.astype(BF)
    for i in range(pieces):
        att_y(i).wait_recv()
    whole = pbuf[core, hi].astype(F32) + abuf[hi].astype(F32) + arecv[...].astype(F32)
    attended[...] = whole.astype(BF)

    @pl.when(me < ep - 1)
    def _():
        k_halo.wait_send()
        v_halo.wait_send()

    for copy in [routes_y, logits_y, tok_y, att_d, mix_y(0), mix_y(1)] + [att_y(i) for i in range(pieces)]:
        copy.wait_send()
    for d in range(ep):
        rd_copy(d).wait_send()
        if d > 0:
            z_copy(d).wait_send()
        if 0 < d < lot:
            n_copy(d).wait_send()
            near_copy(d).wait_send()
        if d >= lot:
            ry_copy(d).wait_send()
            rz_copy(d).wait_send()


def run_fused(dims, tok, gain, routes, logits, sink, qgain, kgain, streams):
    ep, local, cap, rows, width, ffn, own, seq, kv_heads, q_heads, experts = dims
    lot = ep // 2
    order = np.arange(local * 4 * cap)
    e, t, c = order // (4 * cap), order // cap % 4, order % cap
    perm = (t * rows + e * cap + c)[:, None] == np.arange(4 * rows)[None, :]
    perm = jnp.asarray(perm, BF)
    dma = pltpu.SemaphoreType.DMA
    vm = pl.BlockSpec(memory_space=pltpu.VMEM)
    anys = pl.BlockSpec(memory_space=pl.ANY)
    kv_width = kv_heads * 64

    def held(*shape, dtype=BF):
        return pltpu.VMEM(shape, dtype)

    return pl.pallas_call(
        lambda *refs: fused_kernel(dims, *refs),
        name="fused_layer",
        out_shape=(
            jax.ShapeDtypeStruct((own, width), BF), jax.ShapeDtypeStruct((own, width), BF)
        ),
        in_specs=[vm, vm, vm, vm, pl.BlockSpec(memory_space=pltpu.SMEM)] + [vm] * 4 + [anys] * 7,
        out_specs=(vm, vm),
        scratch_shapes=[
            held(q_heads // 2, 128, dtype=F32),
            held(local, width, ffn), held(local, width, ffn), held(local, ffn, width),
            held(q_heads * 64, width),
            held(seq, q_heads * 64),
            held(seq + WINDOW, kv_width), held(seq + WINDOW, kv_width),
            held(kv_heads, seq + WINDOW, 128), held(kv_heads, seq + WINDOW, 128),
            held(seq, q_heads * 64),
            held(ep, rows, width), held(lot, rows, width),
            held(own, width), held(2, own, dtype=jnp.int32), held(2, own, dtype=F32), held(own, width),
            held(ep, 2, 2, rows, width),
            held(local, lot * 4 * cap, width),
            held(ep, 2, rows, width), held(ep, 2, rows, width),
            held(lot, rows, width),
            held(2, lot, rows, width), held(lot, rows, width),
            held(own, width), held(own, width),
            held(2, 2, own, width), held(2, own, width), held(own, width), held(own, width),
            dma((7,)),
            dma((ep,)), dma((ep,)),
            dma((lot,)), dma((lot,)),
            dma((lot,)), dma((lot,)),
            dma((ep,)), dma((ep,)),
            dma((ep,)), dma((ep,)),
            dma((lot,)), dma((lot,)),
            dma((ep,)), dma((ep,)),
            dma((12,)), dma((12,)),
        ],
        compiler_params=pltpu.CompilerParams(
            collective_id=0, has_side_effects=True, vmem_limit_bytes=VMEM_LIMIT
        ),
    )(tok, gain, routes, logits, sink, qgain, kgain, perm, perm.T, *streams)


def fits(dims, tp, kv_size):
    ep, local, cap, rows, width, ffn, own, seq, kv_heads, q_heads, experts = dims
    if tp != 4 or ep < 4 or ep & (ep - 1) or rows % 16 or cap % 4 or kv_size != 64:
        return False
    if own != 128 or seq != 4 * own or kv_heads % 2 or q_heads != 3 * kv_heads or width % 512:
        return False
    lot = ep // 2
    held = 3 * local * width * ffn + q_heads * 64 * width + 3 * seq * q_heads * 64
    held += rows * width * (11 * ep + 5 * lot) + local * lot * 4 * cap * width + 14 * own * width
    return 2 * held < 63 * 1024 * 1024


def on_device(
    query_rows,
    key_rows,
    value_rows,
    query_gain,
    key_gain,
    sink_logits,
    out_weight,
    expert_input,
    expert_gain,
    routes,
    route_logits,
    gate_weight,
    up_weight,
    down_weight,
):
    own_rows = expert_input.shape[0]
    fanout = routes.shape[1]
    capacity = (3 * own_rows * fanout + 2 * EXPERTS - 1) // (2 * EXPERTS)
    ep_size = lax.axis_size("ep")
    tp_size = lax.axis_size("tp")
    local_experts = gate_weight.shape[0]
    key_heads, head_size = key_gain.shape
    dims = (
        ep_size, local_experts, capacity, local_experts * capacity, expert_input.shape[1],
        gate_weight.shape[2], own_rows, query_rows.shape[0], key_heads, query_gain.shape[0],
        EXPERTS,
    )
    if fits(dims, tp_size, head_size):
        return run_fused(
            dims, expert_input, expert_gain.reshape(1, -1), routes.T, route_logits.T,
            sink_logits.reshape(1, -1), query_gain, key_gain,
            (query_rows, key_rows, value_rows, out_weight, gate_weight, up_weight, down_weight),
        )
    heads_out = attend(query_rows, key_rows, value_rows, query_gain, key_gain, sink_logits)
    projected = jnp.dot(heads_out, out_weight, preferred_element_type=jnp.float32).astype(
        jnp.bfloat16
    )
    widened = expert_input.astype(jnp.float32)
    normed = (
        widened
        * lax.rsqrt(jnp.mean(widened * widened, axis=-1, keepdims=True) + EPSILON)
        * expert_gain
    ).astype(jnp.bfloat16)
    route_weight = jax.nn.softmax(route_logits, axis=-1)
    attended = lax.psum_scatter(projected, "tp", scatter_dimension=0, tiled=True)
    combine = combine_matrix(routes, route_weight, capacity)
    sender = dispatch_matrix(routes, capacity)
    slot_rows = jnp.einsum(
        "ecr,rd->ecd", sender, normed, preferred_element_type=jnp.float32
    ).astype(jnp.bfloat16)
    slot_rows = slot_rows.reshape(ep_size, local_experts, capacity, -1)
    arrived = lax.all_to_all(slot_rows, "ep", split_axis=0, concat_axis=0, tiled=True)
    hidden_units = expert_hidden(
        lax.all_gather(arrived, "tp", axis=0, tiled=True), gate_weight, up_weight
    )
    partial_value = jnp.einsum(
        "aecf,efd->aecd", hidden_units, down_weight, preferred_element_type=jnp.float32
    ).astype(jnp.bfloat16)
    partial_value = partial_value.reshape(tp_size, ep_size * local_experts * capacity, -1)
    pieces = lax.all_to_all(partial_value, "tp", split_axis=0, concat_axis=0, tiled=True)
    summed = jnp.sum(pieces, axis=0, dtype=jnp.float32).astype(jnp.bfloat16)
    summed = summed.reshape(ep_size, local_experts * capacity, -1)
    returned = lax.all_to_all(summed, "ep", split_axis=0, concat_axis=0, tiled=True).reshape(
        EXPERTS, capacity, -1
    )
    expert_mix = jnp.einsum(
        "rec,ecd->rd", combine, returned.astype(jnp.float32), precision=lax.Precision.HIGHEST
    ).astype(jnp.bfloat16)
    return (attended, expert_mix)


def solution(mesh):
    placed = (
        P("ep", "tp"),
        P("ep", "tp"),
        P("ep", "tp"),
        P("tp", None),
        P("tp", None),
        P("tp"),
        P("tp", None),
        P(("ep", "tp"), None),
        P(),
        P(("ep", "tp"), None),
        P(("ep", "tp"), None),
        P("ep", None, "tp"),
        P("ep", None, "tp"),
        P("ep", "tp", None),
    )
    return jax.shard_map(
        on_device,
        mesh=mesh,
        in_specs=placed,
        out_specs=(P(("ep", "tp"), None), P(("ep", "tp"), None)),
        check_vma=False,
    )
```

```python
import jax
import jax.numpy as jnp
import numpy as np
from jax import lax
from jax.experimental import pallas as pl
from jax.experimental.pallas import tpu as pltpu
from jax.sharding import PartitionSpec as P

EXPERTS = 32
WINDOW = 128


EPSILON = 1e-06
CLAMP_LIMIT = 7.0
ACT_SLOPE = 1.702
NEGATIVE = -1e30


def shifted(value, axis, steps):
    count = lax.axis_size(axis)
    initial, last = (max(0, -steps), min(count, count - steps))
    return lax.ppermute(value, axis, [(source, source + steps) for source in range(initial, last)])


def head_norm(row_data, gain_table):
    head_count, head_size = gain_table.shape
    widened = row_data.astype(jnp.float32).reshape(row_data.shape[0], head_count, head_size)
    scaled = widened * lax.rsqrt(jnp.mean(widened * widened, axis=-1, keepdims=True) + EPSILON)
    return (scaled * gain_table).astype(jnp.bfloat16)


def band(padded, blocks):
    tiled = padded.reshape((blocks + 1, WINDOW) + padded.shape[1:])
    return jnp.concatenate([tiled[:-1], tiled[1:]], axis=1)


def attend(query_rows, key_rows, value_rows, query_gain, key_gain, sink_logits):
    seq_rows = query_rows.shape[0]
    key_heads, head_size = key_gain.shape
    group_size = query_gain.shape[0] // key_heads
    blocks = seq_rows // WINDOW
    query_hat = head_norm(query_rows, query_gain).reshape(
        blocks, WINDOW, key_heads, group_size, head_size
    )
    key_hat = head_norm(key_rows, key_gain)
    value_hat = value_rows.reshape(seq_rows, key_heads, head_size)
    tail_rows = jnp.stack([key_hat[seq_rows - WINDOW :], value_hat[seq_rows - WINDOW :]])
    earlier = shifted(tail_rows, "ep", 1)
    key_band = band(jnp.concatenate([earlier[0], key_hat], axis=0), blocks)
    value_band = band(jnp.concatenate([earlier[1], value_hat], axis=0), blocks)
    query_pos = lax.broadcasted_iota(jnp.int32, (WINDOW, 2 * WINDOW), 0)
    key_pos = lax.broadcasted_iota(jnp.int32, (WINDOW, 2 * WINDOW), 1)
    distance = query_pos + WINDOW - key_pos
    inside = (distance >= 0) & (distance < WINDOW)
    first_block = (lax.broadcasted_iota(jnp.int32, (blocks, 1, 1), 0) == 0) & (
        lax.axis_index("ep") == 0
    )
    allowed = inside[None] & ~(first_block & (key_pos < WINDOW)[None])
    scores = jnp.einsum(
        "bqkgd,bjkd->bkgqj", query_hat, key_band, preferred_element_type=jnp.float32
    ) * head_size ** (-0.5)
    scores = jnp.where(allowed[:, None, None], scores, NEGATIVE)
    sink_table = sink_logits.reshape(1, key_heads, group_size, 1, 1)
    highest = jnp.maximum(jnp.max(scores, axis=-1, keepdims=True), sink_table)
    weights = jnp.exp(scores - highest)
    total = jnp.sum(weights, axis=-1, keepdims=True) + jnp.exp(sink_table - highest)
    mixed = jnp.einsum(
        "bkgqj,bjkd->bkgqd",
        weights.astype(jnp.bfloat16),
        value_band,
        preferred_element_type=jnp.float32,
    )
    mixed = (mixed / total).astype(jnp.bfloat16)
    return jnp.transpose(mixed, (0, 3, 1, 2, 4)).reshape(seq_rows, -1)


def slot_maps(route_block, capacity):
    flat_routes = route_block.reshape(-1)
    expert_hot = (flat_routes[:, None] == lax.broadcasted_iota(jnp.int32, (1, EXPERTS), 1)).astype(
        jnp.int32
    )
    before = jnp.cumsum(expert_hot, axis=0) - expert_hot
    position = jnp.sum(before * expert_hot, axis=1)
    place_hot = (position[:, None] == lax.broadcasted_iota(jnp.int32, (1, capacity), 1)).astype(
        jnp.float32
    )
    row_total, fanout = route_block.shape
    return (
        expert_hot.astype(jnp.float32).reshape(row_total, fanout, EXPERTS),
        place_hot.reshape(row_total, fanout, capacity),
    )


def dispatch_matrix(route_block, capacity):
    expert_hot, place_hot = slot_maps(route_block, capacity)
    return jnp.einsum("rke,rkc->ecr", expert_hot, place_hot).astype(jnp.bfloat16)


def combine_matrix(route_block, route_weight, capacity):
    expert_hot, place_hot = slot_maps(route_block, capacity)
    return jnp.einsum(
        "rke,rkc,rk->rec", expert_hot, place_hot, route_weight, precision=lax.Precision.HIGHEST
    )


def expert_hidden(piece, gate_weight, up_weight):
    gate_pre = jnp.einsum("aecd,edf->aecf", piece, gate_weight, preferred_element_type=jnp.float32)
    up_pre = jnp.einsum("aecd,edf->aecf", piece, up_weight, preferred_element_type=jnp.float32)
    clipped = jnp.minimum(gate_pre, CLAMP_LIMIT)
    linear = jnp.clip(up_pre, -CLAMP_LIMIT, CLAMP_LIMIT)
    return (clipped * jax.nn.sigmoid(ACT_SLOPE * clipped) * (linear + 1.0)).astype(jnp.bfloat16)


VMEM_LIMIT = 67043328
MESH = pl.DeviceIdType.MESH
BF = jnp.bfloat16
F32 = jnp.float32


def dot(left, right):
    return jnp.dot(left, right, preferred_element_type=F32)


def activation(gate_pre, up_pre):
    clipped = jnp.minimum(gate_pre, CLAMP_LIMIT)
    linear = jnp.clip(up_pre, -CLAMP_LIMIT, CLAMP_LIMIT)
    return (clipped * jax.nn.sigmoid(ACT_SLOPE * clipped) * (linear + 1.0)).astype(BF)


def iota(shape, axis):
    return lax.broadcasted_iota(jnp.int32, shape, axis)


def fused_kernel(
    dims, tok, gain, routes, logits, sink, qgain, kgain, perm, unperm,
    q_hbm, k_hbm, v_hbm, wo_hbm, gate_hbm, up_hbm, down_hbm,
    attended, mixed,
    qpair, gate_w, up_w, down_w, wo, qbuf, kext, vext, kd, vd, ho,
    slots, nslots, ntok, nroutes, nlogits, nrm, gath, xbuf, dbuf, sums, ybuf, retn, retx,
    nsend, nrecv, pbuf, abuf, asend, arecv, partial,
    lsem, zs, zr, ns, nr, ys, yr, ds, dr, rds, rdr, rys, ryr, rzs, rzr, ms, mr,
):
    ep, local, cap, rows, width, ffn, own, seq, kv_heads, q_heads, experts = dims
    lot = ep // 2
    group = 4 * cap
    sorted_rows = 4 * rows
    tile = 512
    pairs = q_heads // 2
    me = lax.axis_index("ep")
    tp = lax.axis_index("tp")
    hi, core = tp // 2, tp % 2
    other = 1 - core
    partner = (me, hi * 2 + other)
    across = (me, (1 - hi) * 2 + core)

    def mate(d):
        found, bit = 0, 1
        while bit < ep:
            found = found + (me // bit + d // bit) % 2 * bit
            bit *= 2
        return found

    inner = (me // (ep // 4) + 1) // 2 % 2

    def far(i):
        return lot + (i + lot // 2) % lot

    def remote(src, dst, send, recv, device):
        return pltpu.make_async_remote_copy(
            src_ref=src, dst_ref=dst, send_sem=send, recv_sem=recv,
            device_id=device, device_id_type=MESH,
        )

    halo = WINDOW
    k_in = pltpu.make_async_copy(k_hbm, kext.at[pl.ds(halo, seq)], lsem.at[0])
    v_in = pltpu.make_async_copy(v_hbm, vext.at[pl.ds(halo, seq)], lsem.at[1])
    q_in = pltpu.make_async_copy(q_hbm, qbuf, lsem.at[2])
    wo_in = pltpu.make_async_copy(wo_hbm, wo, lsem.at[3])
    weights = [
        pltpu.make_async_copy(gate_hbm, gate_w, lsem.at[4]),
        pltpu.make_async_copy(up_hbm, up_w, lsem.at[5]),
        pltpu.make_async_copy(down_hbm, down_w, lsem.at[6]),
    ]

    routes_y = remote(routes, nroutes, ms.at[0], mr.at[0], across)
    logits_y = remote(logits, nlogits, ms.at[5], mr.at[5], across)
    tok_y = remote(tok, ntok, ms.at[1], mr.at[1], across)
    following = ((me + 1) % ep, tp)
    k_halo = remote(
        k_hbm.at[pl.ds(seq - halo, halo)], kext.at[pl.ds(0, halo)], ms.at[2], mr.at[2], following
    )
    v_halo = remote(
        v_hbm.at[pl.ds(seq - halo, halo)], vext.at[pl.ds(0, halo)], ms.at[3], mr.at[3], following
    )
    att_d = remote(pbuf.at[other], abuf, ms.at[4], mr.at[4], partner)
    pieces = 4
    piece = own // pieces

    def att_y(i):
        at = pl.ds(i * piece, piece)
        return remote(asend.at[at], arecv.at[at], ms.at[6 + i], mr.at[6 + i], across)

    def mix_y(i):
        at = pl.ds(i * (own // 2), own // 2)
        return remote(nsend.at[at], nrecv.at[at], ms.at[10 + i], mr.at[10 + i], across)

    def z_copy(d):
        return remote(slots.at[d], gath.at[d, core, hi], zs.at[d], zr.at[d], (mate(d), tp))

    def n_copy(d):
        return remote(nslots.at[d], gath.at[d, core, 1 - hi], ns.at[d], nr.at[d], (mate(d), tp))

    def y_copy(d):
        block = gath.at[d, core, hi]
        return remote(block, block, ys.at[d - lot], yr.at[d - lot], across)

    def d_copy(d):
        block = gath.at[d, core]
        return remote(block, block, ds.at[d], dr.at[d], partner)

    def rd_copy(d):
        return remote(gath.at[d, other], dbuf.at[d], rds.at[d], rdr.at[d], partner)

    def ry_copy(d):
        return remote(
            sums.at[d, 1 - hi], ybuf.at[d - lot], rys.at[d - lot], ryr.at[d - lot], across
        )

    def near_copy(d):
        return remote(sums.at[d], retn.at[:, d], rzs.at[d], rzr.at[d], (mate(d), tp))

    def rz_copy(d):
        return remote(sums.at[d, hi], retx.at[d - lot], rzs.at[d], rzr.at[d], (mate(d), tp))

    def placed(routed, scores):
        table = routed.astype(F32)
        expert_ids = iota((experts, own), 0).astype(F32)
        hot = [(table[k : k + 1] == expert_ids).astype(F32) for k in range(2)]
        earlier = (iota((own, own), 0) < iota((own, own), 1)).astype(BF)
        before = dot((hot[0] + hot[1]).astype(BF), earlier)
        slot = [
            table[k : k + 1] * cap + jnp.sum(before * hot[k], axis=0, keepdims=True)
            for k in range(2)
        ]
        top = jnp.maximum(scores[0:1], scores[1:2])
        raised = [jnp.exp(scores[k : k + 1] - top) for k in range(2)]
        share = [raised[k] / (raised[0] + raised[1]) for k in range(2)]
        return slot, share

    def wanted(first, last, axis):
        count = (last - first) * rows
        shape = (count, 1) if axis == 0 else (1, count)
        place = iota(shape, axis)
        found = place
        for d in range(first, last):
            inside = (place >= (d - first) * rows) & (place < (d - first + 1) * rows)
            found = found + jnp.where(inside, (mate(d) - (d - first)) * rows, 0)
        return found.astype(F32)

    def picker(slot, first, last):
        target = wanted(first, last, 0)
        return ((slot[0] == target) | (slot[1] == target)).astype(BF)

    def column(row):
        diagonal = iota((own, own), 0) == iota((own, own), 1)
        return jnp.sum(jnp.where(diagonal, row, 0.0), axis=1, keepdims=True)

    def combiner(slot, share, first, last):
        target = wanted(first, last, 1)
        full = jnp.where(column(slot[0]) == target, column(share[0]), 0.0)
        full = full + jnp.where(column(slot[1]) == target, column(share[1]), 0.0)
        high = full.astype(BF)
        return high, (full - high.astype(F32)).astype(BF)

    def normalise(source):
        wide = source[...].astype(F32)
        mean = jnp.mean(wide * wide, axis=-1, keepdims=True)
        nrm[...] = (wide * lax.rsqrt(mean + EPSILON) * gain[...]).astype(BF)

    for copy in (k_in, v_in, q_in, wo_in):
        copy.start()
    barrier = pltpu.get_barrier_semaphore()
    for d in range(1, ep):
        pl.semaphore_signal(barrier, inc=1, device_id=(mate(d), tp), device_id_type=MESH)
    pl.semaphore_signal(barrier, inc=1, device_id=across, device_id_type=MESH)
    pl.semaphore_signal(barrier, inc=1, device_id=partner, device_id_type=MESH)

    own_slot, own_share = placed(routes[...], logits[...])
    normalise(tok)
    own_pick = picker(own_slot, 0, ep)
    for col in range(0, width, tile):
        picked = dot(own_pick, nrm[:, col : col + tile]).astype(BF)
        slots[:, :, col : col + tile] = picked.reshape(ep, rows, tile)
        gath[0, core, hi, :, col : col + tile] = picked[:rows]

    pl.semaphore_wait(barrier, ep + 1)
    routes_y.start()
    logits_y.start()
    tok_y.start()

    @pl.when(me < ep - 1)
    def _():
        k_halo.start()
        v_halo.start()

    z_copy(far(0)).start()
    for d in range(1, lot):
        z_copy(d).start()
    for copy in weights:
        copy.start()

    low_half = iota((1, 128), 1) < 64
    same_head = (iota((128, 128), 0) // 64 == iota((128, 128), 1) // 64).astype(BF)

    def gain_pair(table, t):
        return jnp.concatenate([table[2 * t : 2 * t + 1], table[2 * t + 1 : 2 * t + 2]], axis=1)

    for t in range(pairs):
        qpair[t : t + 1] = gain_pair(qgain, t)

    def head_scaled(block, gain_row):
        wide = block.astype(F32)
        square = wide * wide
        high = square.astype(BF)
        rest = (square - high.astype(F32)).astype(BF)
        mean = (dot(high, same_head) + dot(rest, same_head)) * (1.0 / 64.0)
        return wide * lax.rsqrt(mean + EPSILON) * gain_row

    def spread(values, target, m, start, count):
        turned = pltpu.roll(values, 64, 1)
        target[2 * m, pl.ds(start, count)] = jnp.where(low_half, values, turned).astype(BF)
        target[2 * m + 1, pl.ds(start, count)] = jnp.where(low_half, turned, values).astype(BF)

    def prepare(start, count):
        for m in range(kv_heads // 2):
            cols = slice(m * 128, (m + 1) * 128)
            keys = head_scaled(kext[pl.ds(start, count), cols], gain_pair(kgain, m))
            spread(keys.astype(BF).astype(F32), kd, m, start, count)
            spread(vext[pl.ds(start, count), cols].astype(F32), vd, m, start, count)

    share_heads = q_heads // kv_heads

    def attend_pair(b, m):
        top_row = pl.multiple_of(b * WINDOW, WINDOW)
        tiles = share_heads
        low_key = jnp.where((b == 0) & (me == 0), WINDOW, 0)
        query = iota((WINDOW, 2 * WINDOW), 0)
        key = iota((WINDOW, 2 * WINDOW), 1)
        allowed = (key > query) & (key <= query + WINDOW) & (key >= low_key)
        for j in range(tiles):
            lane = pl.multiple_of((m * tiles + j) * 128, 128)
            scaled = head_scaled(
                qbuf[pl.ds(top_row, WINDOW), pl.ds(lane, 128)], qpair[pl.ds(m * tiles + j, 1)]
            ).astype(BF).astype(F32) * 0.125
            outs = []
            for half in range(2):
                head = 2 * j + half
                kv = 2 * m + head // share_heads
                mask = low_half if half == 0 else jnp.logical_not(low_half)
                query_hat = jnp.where(mask, scaled, 0.0).astype(BF)
                keys = kd[kv, pl.ds(top_row, 2 * WINDOW)]
                scores = lax.dot_general(
                    query_hat, keys, (((1,), (1,)), ((), ())), preferred_element_type=F32
                )
                scores = jnp.where(allowed, scores, NEGATIVE)
                sink_value = sink[0, 2 * tiles * m + head]
                highest = jnp.maximum(jnp.max(scores, axis=-1, keepdims=True), sink_value)
                raised = jnp.exp(scores - highest)
                total = jnp.sum(raised, axis=-1, keepdims=True) + jnp.exp(sink_value - highest)
                product = dot(raised.astype(BF), vd[kv, pl.ds(top_row, 2 * WINDOW)])
                outs.append(product / total)
            ho[pl.ds(top_row, WINDOW), pl.ds(lane, 128)] = jnp.where(
                low_half, outs[0], outs[1]
            ).astype(BF)

    k_in.wait()
    v_in.wait()

    @pl.when(me == 0)
    def _():
        kext[0:halo] = jnp.zeros((halo, kext.shape[1]), BF)
        vext[0:halo] = jnp.zeros((halo, vext.shape[1]), BF)

    prepare(halo, seq)
    q_in.wait()
    blocks = seq // WINDOW

    def attend_block(i, carry):
        b = (i + 1) % blocks

        @pl.when(i == blocks - 1)
        def _():
            @pl.when(me > 0)
            def _():
                k_halo.wait_recv()
                v_halo.wait_recv()

            prepare(0, halo)

        lax.fori_loop(0, kv_heads // 2, lambda m, c: (attend_pair(b, m), c)[1], 0)

        return carry

    def forward(d):
        z_copy(d).wait_recv()
        y_copy(d).start()

    def at_edge(step):
        pl.when(inner == 0)(step)

    def at_middle(step):
        pl.when(inner == 1)(step)

    lax.fori_loop(0, blocks, attend_block, 0)
    wo_in.wait()

    def project(i, carry):
        lane = pl.ds(pl.multiple_of(i * 256, 256), 256)
        result = dot(ho[...], wo[:, lane]).astype(BF)
        for t in range(4):
            pbuf[t % 2, t // 2, :, lane] = result[t * own : (t + 1) * own]
        return carry

    lax.fori_loop(0, width // 256, project, 0)
    att_d.start()

    forward(far(0))
    routes_y.wait_recv()
    logits_y.wait_recv()
    tok_y.wait_recv()
    next_slot, next_share = placed(nroutes[...], nlogits[...])
    normalise(ntok)
    next_pick = picker(next_slot, 0, lot)
    for col in range(0, width, tile):
        picked = dot(next_pick, nrm[:, col : col + tile]).astype(BF)
        nslots[:, :, col : col + tile] = picked.reshape(lot, rows, tile)
        gath[0, core, 1 - hi, :, col : col + tile] = picked[:rows]
    for d in range(1, lot):
        n_copy(d).start()
    for i in range(1, lot):
        z_copy(far(i)).start()
    d_copy(0).start()

    att_d.wait_recv()
    asend[...] = (pbuf[core, 1 - hi].astype(F32) + abuf[1 - hi].astype(F32)).astype(BF)
    def arrange(d, at):
        d_copy(d).wait_recv()
        for col in range(0, width, tile):
            block = gath[d, :, :, :, col : col + tile].reshape(sorted_rows, tile)
            moved = dot(perm[...], block).astype(BF)
            for e in range(local):
                xbuf[e, at : at + group, col : col + tile] = moved[e * group : (e + 1) * group]

    def run(at, count, first=0, last=local):
        def expert(e, carry):
            x = xbuf[e, at : at + count]
            hidden = activation(dot(x, gate_w[e]), dot(x, up_w[e]))
            for col in range(0, width, tile):
                xbuf[e, at : at + count, col : col + tile] = dot(
                    hidden, down_w[e, :, col : col + tile]
                ).astype(BF)
            return carry

        lax.fori_loop(first, last, expert, 0)

    def split(d, at, crossed):
        d_copy(d).wait_send()
        if crossed:
            y_copy(d).wait_send()
        for col in range(0, width, tile):
            block = jnp.concatenate(
                [xbuf[e, at : at + group, col : col + tile] for e in range(local)], axis=0
            )
            back = dot(unperm[...], block).astype(BF)
            gath[d, :, :, :, col : col + tile] = back.reshape(2, 2, rows, tile)
        rd_copy(d).start()

    def join(d):
        rd_copy(d).wait_recv()
        part = gath[d, core, 1 - hi].astype(F32) + dbuf[d, 1 - hi].astype(F32)
        sums[d, 1 - hi] = part.astype(BF)
        ry_copy(d).start()

    def near_join(d):
        rd_copy(d).wait_recv()
        for h in range(2):
            part = (gath[d, core, h].astype(F32) + dbuf[d, h].astype(F32)).astype(BF)
            if d == 0:
                retn[h, 0] = part
            else:
                sums[d, h] = part
        if d > 0:
            near_copy(d).start()

    def finish(d):
        ry_copy(d).wait_recv()
        total = gath[d, core, hi].astype(F32) + dbuf[d, hi].astype(F32)
        sums[d, hi] = (total + ybuf[d - lot].astype(F32)).astype(BF)
        rz_copy(d).start()

    def hand_over(d):
        y_copy(d).wait_recv()
        d_copy(d).start()

    def near_hand_over(d):
        z_copy(d).wait_recv()
        n_copy(d).wait_recv()
        d_copy(d).start()

    def near_sum():
        near_pick = combiner(next_slot, next_share, 0, lot)
        for d in range(1, lot):
            near_copy(d).wait_recv()
        for col in range(0, width, tile):
            near = retn[1 - hi, :, :, col : col + tile].reshape(lot * rows, tile)
            total = dot(near_pick[0], near) + dot(near_pick[1], near)
            nsend[:, col : col + tile] = total.astype(BF)
        for i in range(2):
            mix_y(i).start()

    att_y(0).start()
    att_y(1).start()
    for copy in weights:
        copy.wait()
    hand_over(far(0))
    arrange(far(0), 0)
    run(0, group)
    split(far(0), 0, True)
    for d in range(1, lot):
        near_hand_over(d)
    arrange(0, 0)
    join(far(0))
    forward(far(1))
    for d in range(1, lot):
        arrange(d, d * group)
    run(0, lot * group, 0, 2)
    run(0, lot * group, 2, 3)
    forward(far(2))
    finish(far(0))
    run(0, lot * group, 3, 4)
    for d in range(1, lot):
        split(d, d * group, False)
    hand_over(far(1))
    split(0, 0, False)
    forward(far(3))
    for d in range(1, lot):
        near_join(d)
    att_y(2).start()
    att_y(3).start()
    arrange(far(1), 0)
    hand_over(far(2))
    near_join(0)
    arrange(far(2), group)
    run(0, 2 * group)
    hand_over(far(3))
    split(far(1), 0, True)
    split(far(2), group, True)
    arrange(far(3), 0)
    join(far(1))
    join(far(2))
    run(0, group, 0, 2)
    finish(far(1))
    run(0, group, 2, 4)
    split(far(3), 0, True)
    finish(far(2))
    join(far(3))
    near_sum()
    finish(far(3))

    half = lot // 2
    own_near = combiner(own_slot, own_share, 0, lot)
    own_late = combiner(own_slot, own_share, lot, lot + half)
    own_early = combiner(own_slot, own_share, lot + half, ep)
    for i in range(half):
        rz_copy(far(i)).wait_recv()
    for col in range(0, width, tile):
        near = retn[hi, :, :, col : col + tile].reshape(lot * rows, tile)
        early = retx[half:, :, col : col + tile].reshape(half * rows, tile)
        total = dot(own_near[0], near) + dot(own_near[1], near)
        total = total + dot(own_early[0], early) + dot(own_early[1], early)
        partial[:, col : col + tile] = total
    for i in range(pieces):
        att_y(i).wait_recv()
    whole = pbuf[core, hi].astype(F32) + abuf[hi].astype(F32) + arecv[...].astype(F32)
    attended[...] = whole.astype(BF)
    for i in range(half, lot):
        rz_copy(far(i)).wait_recv()
    for i in range(2):
        mix_y(i).wait_recv()
    for col in range(0, width, tile):
        late = retx[:half, :, col : col + tile].reshape(half * rows, tile)
        total = partial[:, col : col + tile] + nrecv[:, col : col + tile].astype(F32)
        total = total + dot(own_late[0], late) + dot(own_late[1], late)
        mixed[:, col : col + tile] = total.astype(BF)

    @pl.when(me < ep - 1)
    def _():
        k_halo.wait_send()
        v_halo.wait_send()

    for copy in [routes_y, logits_y, tok_y, att_d, mix_y(0), mix_y(1)] + [att_y(i) for i in range(pieces)]:
        copy.wait_send()
    for d in range(ep):
        rd_copy(d).wait_send()
        if d > 0:
            z_copy(d).wait_send()
        if 0 < d < lot:
            n_copy(d).wait_send()
            near_copy(d).wait_send()
        if d >= lot:
            ry_copy(d).wait_send()
            rz_copy(d).wait_send()


def run_fused(dims, tok, gain, routes, logits, sink, qgain, kgain, streams):
    ep, local, cap, rows, width, ffn, own, seq, kv_heads, q_heads, experts = dims
    lot = ep // 2
    order = np.arange(local * 4 * cap)
    e, t, c = order // (4 * cap), order // cap % 4, order % cap
    perm = (t * rows + e * cap + c)[:, None] == np.arange(4 * rows)[None, :]
    perm = jnp.asarray(perm, BF)
    dma = pltpu.SemaphoreType.DMA
    vm = pl.BlockSpec(memory_space=pltpu.VMEM)
    anys = pl.BlockSpec(memory_space=pl.ANY)
    kv_width = kv_heads * 64

    def held(*shape, dtype=BF):
        return pltpu.VMEM(shape, dtype)

    return pl.pallas_call(
        lambda *refs: fused_kernel(dims, *refs),
        name="fused_layer",
        out_shape=(
            jax.ShapeDtypeStruct((own, width), BF), jax.ShapeDtypeStruct((own, width), BF)
        ),
        in_specs=[vm, vm, vm, vm, pl.BlockSpec(memory_space=pltpu.SMEM)] + [vm] * 4 + [anys] * 7,
        out_specs=(vm, vm),
        scratch_shapes=[
            held(q_heads // 2, 128, dtype=F32),
            held(local, width, ffn), held(local, width, ffn), held(local, ffn, width),
            held(q_heads * 64, width),
            held(seq, q_heads * 64),
            held(seq + WINDOW, kv_width), held(seq + WINDOW, kv_width),
            held(kv_heads, seq + WINDOW, 128), held(kv_heads, seq + WINDOW, 128),
            held(seq, q_heads * 64),
            held(ep, rows, width), held(lot, rows, width),
            held(own, width), held(2, own, dtype=jnp.int32), held(2, own, dtype=F32), held(own, width),
            held(ep, 2, 2, rows, width),
            held(local, lot * 4 * cap, width),
            held(ep, 2, rows, width), held(ep, 2, rows, width),
            held(lot, rows, width),
            held(2, lot, rows, width), held(lot, rows, width),
            held(own, width), held(own, width),
            held(2, 2, own, width), held(2, own, width), held(own, width), held(own, width),
            held(own, width, dtype=F32),
            dma((7,)),
            dma((ep,)), dma((ep,)),
            dma((lot,)), dma((lot,)),
            dma((lot,)), dma((lot,)),
            dma((ep,)), dma((ep,)),
            dma((ep,)), dma((ep,)),
            dma((lot,)), dma((lot,)),
            dma((ep,)), dma((ep,)),
            dma((12,)), dma((12,)),
        ],
        compiler_params=pltpu.CompilerParams(
            collective_id=0, has_side_effects=True, vmem_limit_bytes=VMEM_LIMIT
        ),
    )(tok, gain, routes, logits, sink, qgain, kgain, perm, perm.T, *streams)


def hand_out(first, second):
    count = 2
    rows, width = first.shape
    piece = rows // count

    def kernel(first_in, second_in, first_out, second_out, held, sem_in, sem_out):
        pairs = ((first_in, first_out), (second_in, second_out))
        steps = [(a, i) for a in range(2) for i in range(count)]

        def inward(a, i):
            at = pl.ds(i * piece, piece)
            return pltpu.make_async_copy(pairs[a][0].at[at], held.at[a, at], sem_in.at[a, i])

        def outward(a, i):
            at = pl.ds(i * piece, piece)
            return pltpu.make_async_copy(held.at[a, at], pairs[a][1].at[at], sem_out.at[a, i])

        for step in steps:
            inward(*step).start()
        for step in steps:
            inward(*step).wait()
            outward(*step).start()
        for step in steps:
            outward(*step).wait()

    anys = pl.BlockSpec(memory_space=pl.ANY)
    shape = jax.ShapeDtypeStruct(first.shape, first.dtype)
    return pl.pallas_call(
        kernel,
        name="hand_out",
        out_shape=(shape, shape),
        in_specs=[anys, anys],
        out_specs=(anys, anys),
        scratch_shapes=[
            pltpu.VMEM((2, rows, width), BF),
            pltpu.SemaphoreType.DMA((2, count)),
            pltpu.SemaphoreType.DMA((2, count)),
        ],
    )(first, second)


def fits(dims, tp, kv_size):
    ep, local, cap, rows, width, ffn, own, seq, kv_heads, q_heads, experts = dims
    if tp != 4 or ep < 4 or ep & (ep - 1) or rows % 16 or cap % 4 or kv_size != 64:
        return False
    if own != 128 or seq != 4 * own or kv_heads % 2 or q_heads != 3 * kv_heads or width % 512:
        return False
    lot = ep // 2
    held = 3 * local * width * ffn + q_heads * 64 * width + 3 * seq * q_heads * 64
    held += rows * width * (11 * ep + 5 * lot) + local * lot * 4 * cap * width + 16 * own * width
    return 2 * held < 63 * 1024 * 1024


def on_device(
    query_rows,
    key_rows,
    value_rows,
    query_gain,
    key_gain,
    sink_logits,
    out_weight,
    expert_input,
    expert_gain,
    routes,
    route_logits,
    gate_weight,
    up_weight,
    down_weight,
):
    own_rows = expert_input.shape[0]
    fanout = routes.shape[1]
    capacity = (3 * own_rows * fanout + 2 * EXPERTS - 1) // (2 * EXPERTS)
    ep_size = lax.axis_size("ep")
    tp_size = lax.axis_size("tp")
    local_experts = gate_weight.shape[0]
    key_heads, head_size = key_gain.shape
    dims = (
        ep_size, local_experts, capacity, local_experts * capacity, expert_input.shape[1],
        gate_weight.shape[2], own_rows, query_rows.shape[0], key_heads, query_gain.shape[0],
        EXPERTS,
    )
    if fits(dims, tp_size, head_size):
        results = run_fused(
            dims, expert_input, expert_gain.reshape(1, -1), routes.T, route_logits.T,
            sink_logits.reshape(1, -1), query_gain, key_gain,
            (query_rows, key_rows, value_rows, out_weight, gate_weight, up_weight, down_weight),
        )
        return hand_out(*results)
    heads_out = attend(query_rows, key_rows, value_rows, query_gain, key_gain, sink_logits)
    projected = jnp.dot(heads_out, out_weight, preferred_element_type=jnp.float32).astype(
        jnp.bfloat16
    )
    widened = expert_input.astype(jnp.float32)
    normed = (
        widened
        * lax.rsqrt(jnp.mean(widened * widened, axis=-1, keepdims=True) + EPSILON)
        * expert_gain
    ).astype(jnp.bfloat16)
    route_weight = jax.nn.softmax(route_logits, axis=-1)
    attended = lax.psum_scatter(projected, "tp", scatter_dimension=0, tiled=True)
    combine = combine_matrix(routes, route_weight, capacity)
    sender = dispatch_matrix(routes, capacity)
    slot_rows = jnp.einsum(
        "ecr,rd->ecd", sender, normed, preferred_element_type=jnp.float32
    ).astype(jnp.bfloat16)
    slot_rows = slot_rows.reshape(ep_size, local_experts, capacity, -1)
    arrived = lax.all_to_all(slot_rows, "ep", split_axis=0, concat_axis=0, tiled=True)
    hidden_units = expert_hidden(
        lax.all_gather(arrived, "tp", axis=0, tiled=True), gate_weight, up_weight
    )
    partial_value = jnp.einsum(
        "aecf,efd->aecd", hidden_units, down_weight, preferred_element_type=jnp.float32
    ).astype(jnp.bfloat16)
    partial_value = partial_value.reshape(tp_size, ep_size * local_experts * capacity, -1)
    pieces = lax.all_to_all(partial_value, "tp", split_axis=0, concat_axis=0, tiled=True)
    summed = jnp.sum(pieces, axis=0, dtype=jnp.float32).astype(jnp.bfloat16)
    summed = summed.reshape(ep_size, local_experts * capacity, -1)
    returned = lax.all_to_all(summed, "ep", split_axis=0, concat_axis=0, tiled=True).reshape(
        EXPERTS, capacity, -1
    )
    expert_mix = jnp.einsum(
        "rec,ecd->rd", combine, returned.astype(jnp.float32), precision=lax.Precision.HIGHEST
    ).astype(jnp.bfloat16)
    return (attended, expert_mix)


def solution(mesh):
    placed = (
        P("ep", "tp"),
        P("ep", "tp"),
        P("ep", "tp"),
        P("tp", None),
        P("tp", None),
        P("tp"),
        P("tp", None),
        P(("ep", "tp"), None),
        P(),
        P(("ep", "tp"), None),
        P(("ep", "tp"), None),
        P("ep", None, "tp"),
        P("ep", None, "tp"),
        P("ep", "tp", None),
    )
    return jax.shard_map(
        on_device,
        mesh=mesh,
        in_specs=placed,
        out_specs=(P(("ep", "tp"), None), P(("ep", "tp"), None)),
        check_vma=False,
    )
```

```python
import jax
import jax.numpy as jnp
import numpy as np
from jax import lax
from jax.experimental import pallas as pl
from jax.experimental.pallas import tpu as pltpu
from jax.sharding import PartitionSpec as P

EXPERTS = 32
WINDOW = 128


EPSILON = 1e-06
CLAMP_LIMIT = 7.0
ACT_SLOPE = 1.702
NEGATIVE = -1e30


def shifted(value, axis, steps):
    count = lax.axis_size(axis)
    initial, last = (max(0, -steps), min(count, count - steps))
    return lax.ppermute(value, axis, [(source, source + steps) for source in range(initial, last)])


def head_norm(row_data, gain_table):
    head_count, head_size = gain_table.shape
    widened = row_data.astype(jnp.float32).reshape(row_data.shape[0], head_count, head_size)
    scaled = widened * lax.rsqrt(jnp.mean(widened * widened, axis=-1, keepdims=True) + EPSILON)
    return (scaled * gain_table).astype(jnp.bfloat16)


def band(padded, blocks):
    tiled = padded.reshape((blocks + 1, WINDOW) + padded.shape[1:])
    return jnp.concatenate([tiled[:-1], tiled[1:]], axis=1)


def attend(query_rows, key_rows, value_rows, query_gain, key_gain, sink_logits):
    seq_rows = query_rows.shape[0]
    key_heads, head_size = key_gain.shape
    group_size = query_gain.shape[0] // key_heads
    blocks = seq_rows // WINDOW
    query_hat = head_norm(query_rows, query_gain).reshape(
        blocks, WINDOW, key_heads, group_size, head_size
    )
    key_hat = head_norm(key_rows, key_gain)
    value_hat = value_rows.reshape(seq_rows, key_heads, head_size)
    tail_rows = jnp.stack([key_hat[seq_rows - WINDOW :], value_hat[seq_rows - WINDOW :]])
    earlier = shifted(tail_rows, "ep", 1)
    key_band = band(jnp.concatenate([earlier[0], key_hat], axis=0), blocks)
    value_band = band(jnp.concatenate([earlier[1], value_hat], axis=0), blocks)
    query_pos = lax.broadcasted_iota(jnp.int32, (WINDOW, 2 * WINDOW), 0)
    key_pos = lax.broadcasted_iota(jnp.int32, (WINDOW, 2 * WINDOW), 1)
    distance = query_pos + WINDOW - key_pos
    inside = (distance >= 0) & (distance < WINDOW)
    first_block = (lax.broadcasted_iota(jnp.int32, (blocks, 1, 1), 0) == 0) & (
        lax.axis_index("ep") == 0
    )
    allowed = inside[None] & ~(first_block & (key_pos < WINDOW)[None])
    scores = jnp.einsum(
        "bqkgd,bjkd->bkgqj", query_hat, key_band, preferred_element_type=jnp.float32
    ) * head_size ** (-0.5)
    scores = jnp.where(allowed[:, None, None], scores, NEGATIVE)
    sink_table = sink_logits.reshape(1, key_heads, group_size, 1, 1)
    highest = jnp.maximum(jnp.max(scores, axis=-1, keepdims=True), sink_table)
    weights = jnp.exp(scores - highest)
    total = jnp.sum(weights, axis=-1, keepdims=True) + jnp.exp(sink_table - highest)
    mixed = jnp.einsum(
        "bkgqj,bjkd->bkgqd",
        weights.astype(jnp.bfloat16),
        value_band,
        preferred_element_type=jnp.float32,
    )
    mixed = (mixed / total).astype(jnp.bfloat16)
    return jnp.transpose(mixed, (0, 3, 1, 2, 4)).reshape(seq_rows, -1)


def slot_maps(route_block, capacity):
    flat_routes = route_block.reshape(-1)
    expert_hot = (flat_routes[:, None] == lax.broadcasted_iota(jnp.int32, (1, EXPERTS), 1)).astype(
        jnp.int32
    )
    before = jnp.cumsum(expert_hot, axis=0) - expert_hot
    position = jnp.sum(before * expert_hot, axis=1)
    place_hot = (position[:, None] == lax.broadcasted_iota(jnp.int32, (1, capacity), 1)).astype(
        jnp.float32
    )
    row_total, fanout = route_block.shape
    return (
        expert_hot.astype(jnp.float32).reshape(row_total, fanout, EXPERTS),
        place_hot.reshape(row_total, fanout, capacity),
    )


def dispatch_matrix(route_block, capacity):
    expert_hot, place_hot = slot_maps(route_block, capacity)
    return jnp.einsum("rke,rkc->ecr", expert_hot, place_hot).astype(jnp.bfloat16)


def combine_matrix(route_block, route_weight, capacity):
    expert_hot, place_hot = slot_maps(route_block, capacity)
    return jnp.einsum(
        "rke,rkc,rk->rec", expert_hot, place_hot, route_weight, precision=lax.Precision.HIGHEST
    )


def expert_hidden(piece, gate_weight, up_weight):
    gate_pre = jnp.einsum("aecd,edf->aecf", piece, gate_weight, preferred_element_type=jnp.float32)
    up_pre = jnp.einsum("aecd,edf->aecf", piece, up_weight, preferred_element_type=jnp.float32)
    clipped = jnp.minimum(gate_pre, CLAMP_LIMIT)
    linear = jnp.clip(up_pre, -CLAMP_LIMIT, CLAMP_LIMIT)
    return (clipped * jax.nn.sigmoid(ACT_SLOPE * clipped) * (linear + 1.0)).astype(jnp.bfloat16)


VMEM_LIMIT = 67043328
MESH = pl.DeviceIdType.MESH
BF = jnp.bfloat16
F32 = jnp.float32


def dot(left, right):
    return jnp.dot(left, right, preferred_element_type=F32)


def activation(gate_pre, up_pre):
    clipped = jnp.minimum(gate_pre, CLAMP_LIMIT)
    linear = jnp.clip(up_pre, -CLAMP_LIMIT, CLAMP_LIMIT)
    return (clipped * jax.nn.sigmoid(ACT_SLOPE * clipped) * (linear + 1.0)).astype(BF)


def iota(shape, axis):
    return lax.broadcasted_iota(jnp.int32, shape, axis)


def fused_kernel(
    dims, tok_in, gain_in, routes_in, logits_in, sink_in, qgain_in, kgain_in, perm_in, unperm_in,
    q_hbm, k_hbm, v_hbm, wo_hbm, gate_hbm, up_hbm, down_hbm,
    attended, mixed,
    tok, gain, routes, logits, sink, qgain, kgain, perm, unperm,
    qpair, gate_w, up_w, down_w, wo, qbuf, kext, vext, kd, vd, ho,
    slots, nslots, ntok, nroutes, nlogits, nrm, gath, xbuf, dbuf, sums, ybuf, retn, retx,
    nsend, nrecv, pbuf, abuf, asend, arecv, partial,
    lsem, zs, zr, ns, nr, ys, yr, ds, dr, rds, rdr, rys, ryr, rzs, rzr, ms, mr,
):
    ep, local, cap, rows, width, ffn, own, seq, kv_heads, q_heads, experts = dims
    lot = ep // 2
    group = 4 * cap
    sorted_rows = 4 * rows
    tile = 512
    pairs = q_heads // 2
    me = lax.axis_index("ep")
    tp = lax.axis_index("tp")
    hi, core = tp // 2, tp % 2
    other = 1 - core
    partner = (me, hi * 2 + other)
    across = (me, (1 - hi) * 2 + core)

    def mate(d):
        found, bit = 0, 1
        while bit < ep:
            found = found + (me // bit + d // bit) % 2 * bit
            bit *= 2
        return found

    inner = (me // (ep // 4) + 1) // 2 % 2

    def far(i):
        return lot + (i + lot // 2) % lot

    def remote(src, dst, send, recv, device):
        return pltpu.make_async_remote_copy(
            src_ref=src, dst_ref=dst, send_sem=send, recv_sem=recv,
            device_id=device, device_id_type=MESH,
        )

    halo = WINDOW
    k_in = pltpu.make_async_copy(k_hbm, kext.at[pl.ds(halo, seq)], lsem.at[0])
    v_in = pltpu.make_async_copy(v_hbm, vext.at[pl.ds(halo, seq)], lsem.at[1])
    q_in = pltpu.make_async_copy(q_hbm, qbuf, lsem.at[2])
    wo_in = pltpu.make_async_copy(wo_hbm, wo, lsem.at[3])
    weights = [
        pltpu.make_async_copy(gate_hbm, gate_w, lsem.at[4]),
        pltpu.make_async_copy(up_hbm, up_w, lsem.at[5]),
        pltpu.make_async_copy(down_hbm, down_w, lsem.at[6]),
    ]

    routes_y = remote(routes, nroutes, ms.at[0], mr.at[0], across)
    logits_y = remote(logits, nlogits, ms.at[5], mr.at[5], across)
    tok_y = remote(tok, ntok, ms.at[1], mr.at[1], across)
    following = ((me + 1) % ep, tp)
    k_halo = remote(
        k_hbm.at[pl.ds(seq - halo, halo)], kext.at[pl.ds(0, halo)], ms.at[2], mr.at[2], following
    )
    v_halo = remote(
        v_hbm.at[pl.ds(seq - halo, halo)], vext.at[pl.ds(0, halo)], ms.at[3], mr.at[3], following
    )
    att_d = remote(pbuf.at[other], abuf, ms.at[4], mr.at[4], partner)
    pieces = 4
    piece = own // pieces

    def att_y(i):
        at = pl.ds(i * piece, piece)
        return remote(asend.at[at], arecv.at[at], ms.at[6 + i], mr.at[6 + i], across)

    def mix_y(i):
        at = pl.ds(i * (own // 2), own // 2)
        return remote(nsend.at[at], nrecv.at[at], ms.at[10 + i], mr.at[10 + i], across)

    def z_copy(d):
        return remote(slots.at[d], gath.at[d, core, hi], zs.at[d], zr.at[d], (mate(d), tp))

    def n_copy(d):
        return remote(nslots.at[d], gath.at[d, core, 1 - hi], ns.at[d], nr.at[d], (mate(d), tp))

    def y_copy(d):
        block = gath.at[d, core, hi]
        return remote(block, block, ys.at[d - lot], yr.at[d - lot], across)

    def d_copy(d):
        block = gath.at[d, core]
        return remote(block, block, ds.at[d], dr.at[d], partner)

    def rd_copy(d):
        return remote(gath.at[d, other], dbuf.at[d], rds.at[d], rdr.at[d], partner)

    def ry_copy(d):
        return remote(
            sums.at[d, 1 - hi], ybuf.at[d - lot], rys.at[d - lot], ryr.at[d - lot], across
        )

    def near_copy(d):
        return remote(sums.at[d], retn.at[:, d], rzs.at[d], rzr.at[d], (mate(d), tp))

    def rz_copy(d):
        return remote(sums.at[d, hi], retx.at[d - lot], rzs.at[d], rzr.at[d], (mate(d), tp))

    def placed(routed, scores):
        table = routed.astype(F32)
        expert_ids = iota((experts, own), 0).astype(F32)
        hot = [(table[k : k + 1] == expert_ids).astype(F32) for k in range(2)]
        earlier = (iota((own, own), 0) < iota((own, own), 1)).astype(BF)
        before = dot((hot[0] + hot[1]).astype(BF), earlier)
        slot = [
            table[k : k + 1] * cap + jnp.sum(before * hot[k], axis=0, keepdims=True)
            for k in range(2)
        ]
        top = jnp.maximum(scores[0:1], scores[1:2])
        raised = [jnp.exp(scores[k : k + 1] - top) for k in range(2)]
        share = [raised[k] / (raised[0] + raised[1]) for k in range(2)]
        return slot, share

    def wanted(first, last, axis):
        count = (last - first) * rows
        shape = (count, 1) if axis == 0 else (1, count)
        place = iota(shape, axis)
        found = place
        for d in range(first, last):
            inside = (place >= (d - first) * rows) & (place < (d - first + 1) * rows)
            found = found + jnp.where(inside, (mate(d) - (d - first)) * rows, 0)
        return found.astype(F32)

    def picker(slot, first, last):
        target = wanted(first, last, 0)
        return ((slot[0] == target) | (slot[1] == target)).astype(BF)

    def column(row):
        diagonal = iota((own, own), 0) == iota((own, own), 1)
        return jnp.sum(jnp.where(diagonal, row, 0.0), axis=1, keepdims=True)

    def combiner(slot, share, first, last):
        target = wanted(first, last, 1)
        full = jnp.where(column(slot[0]) == target, column(share[0]), 0.0)
        full = full + jnp.where(column(slot[1]) == target, column(share[1]), 0.0)
        high = full.astype(BF)
        return high, (full - high.astype(F32)).astype(BF)

    def normalise(source):
        wide = source[...].astype(F32)
        mean = jnp.mean(wide * wide, axis=-1, keepdims=True)
        nrm[...] = (wide * lax.rsqrt(mean + EPSILON) * gain[...]).astype(BF)

    sources = (
        tok_in, routes_in, logits_in, gain_in, sink_in, qgain_in, kgain_in, perm_in, unperm_in
    )
    targets = (tok, routes, logits, gain, sink, qgain, kgain, perm, unperm)
    small = [
        pltpu.make_async_copy(source, target, lsem.at[7 + i])
        for i, (source, target) in enumerate(zip(sources, targets))
    ]
    for copy in small:
        copy.start()
    barrier = pltpu.get_barrier_semaphore()
    for d in range(1, ep):
        pl.semaphore_signal(barrier, inc=1, device_id=(mate(d), tp), device_id_type=MESH)
    pl.semaphore_signal(barrier, inc=1, device_id=across, device_id_type=MESH)
    pl.semaphore_signal(barrier, inc=1, device_id=partner, device_id_type=MESH)

    for copy in (k_in, v_in, q_in, wo_in):
        copy.start()
    for copy in small:
        copy.wait()
    own_slot, own_share = placed(routes[...], logits[...])
    normalise(tok)
    own_pick = picker(own_slot, 0, ep)
    for col in range(0, width, tile):
        picked = dot(own_pick, nrm[:, col : col + tile]).astype(BF)
        slots[:, :, col : col + tile] = picked.reshape(ep, rows, tile)
        gath[0, core, hi, :, col : col + tile] = picked[:rows]

    pl.semaphore_wait(barrier, ep + 1)
    routes_y.start()
    logits_y.start()
    tok_y.start()

    @pl.when(me < ep - 1)
    def _():
        k_halo.start()
        v_halo.start()

    z_copy(far(0)).start()
    for d in range(1, lot):
        z_copy(d).start()
    for copy in weights:
        copy.start()

    low_half = iota((1, 128), 1) < 64
    same_head = (iota((128, 128), 0) // 64 == iota((128, 128), 1) // 64).astype(BF)

    def gain_pair(table, t):
        return jnp.concatenate([table[2 * t : 2 * t + 1], table[2 * t + 1 : 2 * t + 2]], axis=1)

    for t in range(pairs):
        qpair[t : t + 1] = gain_pair(qgain, t)

    def head_scaled(block, gain_row):
        wide = block.astype(F32)
        square = wide * wide
        high = square.astype(BF)
        rest = (square - high.astype(F32)).astype(BF)
        mean = (dot(high, same_head) + dot(rest, same_head)) * (1.0 / 64.0)
        return wide * lax.rsqrt(mean + EPSILON) * gain_row

    def spread(values, target, m, start, count):
        turned = pltpu.roll(values, 64, 1)
        target[2 * m, pl.ds(start, count)] = jnp.where(low_half, values, turned).astype(BF)
        target[2 * m + 1, pl.ds(start, count)] = jnp.where(low_half, turned, values).astype(BF)

    def prepare(start, count):
        for m in range(kv_heads // 2):
            cols = slice(m * 128, (m + 1) * 128)
            keys = head_scaled(kext[pl.ds(start, count), cols], gain_pair(kgain, m))
            spread(keys.astype(BF).astype(F32), kd, m, start, count)
            spread(vext[pl.ds(start, count), cols].astype(F32), vd, m, start, count)

    share_heads = q_heads // kv_heads

    def attend_pair(b, m):
        top_row = pl.multiple_of(b * WINDOW, WINDOW)
        tiles = share_heads
        low_key = jnp.where((b == 0) & (me == 0), WINDOW, 0)
        query = iota((WINDOW, 2 * WINDOW), 0)
        key = iota((WINDOW, 2 * WINDOW), 1)
        allowed = (key > query) & (key <= query + WINDOW) & (key >= low_key)
        for j in range(tiles):
            lane = pl.multiple_of((m * tiles + j) * 128, 128)
            scaled = head_scaled(
                qbuf[pl.ds(top_row, WINDOW), pl.ds(lane, 128)], qpair[pl.ds(m * tiles + j, 1)]
            ).astype(BF).astype(F32) * 0.125
            outs = []
            for half in range(2):
                head = 2 * j + half
                kv = 2 * m + head // share_heads
                mask = low_half if half == 0 else jnp.logical_not(low_half)
                query_hat = jnp.where(mask, scaled, 0.0).astype(BF)
                keys = kd[kv, pl.ds(top_row, 2 * WINDOW)]
                scores = lax.dot_general(
                    query_hat, keys, (((1,), (1,)), ((), ())), preferred_element_type=F32
                )
                scores = jnp.where(allowed, scores, NEGATIVE)
                sink_value = sink[0, 2 * tiles * m + head]
                highest = jnp.maximum(jnp.max(scores, axis=-1, keepdims=True), sink_value)
                raised = jnp.exp(scores - highest)
                total = jnp.sum(raised, axis=-1, keepdims=True) + jnp.exp(sink_value - highest)
                product = dot(raised.astype(BF), vd[kv, pl.ds(top_row, 2 * WINDOW)])
                outs.append(product / total)
            ho[pl.ds(top_row, WINDOW), pl.ds(lane, 128)] = jnp.where(
                low_half, outs[0], outs[1]
            ).astype(BF)

    k_in.wait()
    v_in.wait()

    @pl.when(me == 0)
    def _():
        kext[0:halo] = jnp.zeros((halo, kext.shape[1]), BF)
        vext[0:halo] = jnp.zeros((halo, vext.shape[1]), BF)

    prepare(halo, seq)
    q_in.wait()
    blocks = seq // WINDOW

    def attend_block(i, carry):
        b = (i + 1) % blocks

        @pl.when(i == blocks - 1)
        def _():
            @pl.when(me > 0)
            def _():
                k_halo.wait_recv()
                v_halo.wait_recv()

            prepare(0, halo)

        lax.fori_loop(0, kv_heads // 2, lambda m, c: (attend_pair(b, m), c)[1], 0)

        return carry

    def forward(d):
        z_copy(d).wait_recv()
        y_copy(d).start()

    def at_edge(step):
        pl.when(inner == 0)(step)

    def at_middle(step):
        pl.when(inner == 1)(step)

    lax.fori_loop(0, blocks, attend_block, 0)
    wo_in.wait()

    def project(i, carry):
        lane = pl.ds(pl.multiple_of(i * 256, 256), 256)
        result = dot(ho[...], wo[:, lane]).astype(BF)
        for t in range(4):
            pbuf[t % 2, t // 2, :, lane] = result[t * own : (t + 1) * own]
        return carry

    lax.fori_loop(0, width // 256, project, 0)
    att_d.start()

    forward(far(0))
    routes_y.wait_recv()
    logits_y.wait_recv()
    tok_y.wait_recv()
    next_slot, next_share = placed(nroutes[...], nlogits[...])
    normalise(ntok)
    next_pick = picker(next_slot, 0, lot)
    for col in range(0, width, tile):
        picked = dot(next_pick, nrm[:, col : col + tile]).astype(BF)
        nslots[:, :, col : col + tile] = picked.reshape(lot, rows, tile)
        gath[0, core, 1 - hi, :, col : col + tile] = picked[:rows]
    for d in range(1, lot):
        n_copy(d).start()
    for i in range(1, lot):
        z_copy(far(i)).start()
    d_copy(0).start()

    att_d.wait_recv()
    asend[...] = (pbuf[core, 1 - hi].astype(F32) + abuf[1 - hi].astype(F32)).astype(BF)
    def arrange(d, at):
        d_copy(d).wait_recv()
        for col in range(0, width, tile):
            block = gath[d, :, :, :, col : col + tile].reshape(sorted_rows, tile)
            moved = dot(perm[...], block).astype(BF)
            for e in range(local):
                xbuf[e, at : at + group, col : col + tile] = moved[e * group : (e + 1) * group]

    def run(at, count, first=0, last=local):
        def expert(e, carry):
            x = xbuf[e, at : at + count]
            hidden = activation(dot(x, gate_w[e]), dot(x, up_w[e]))
            for col in range(0, width, tile):
                xbuf[e, at : at + count, col : col + tile] = dot(
                    hidden, down_w[e, :, col : col + tile]
                ).astype(BF)
            return carry

        lax.fori_loop(first, last, expert, 0)

    def split(d, at, crossed):
        d_copy(d).wait_send()
        if crossed:
            y_copy(d).wait_send()
        for col in range(0, width, tile):
            block = jnp.concatenate(
                [xbuf[e, at : at + group, col : col + tile] for e in range(local)], axis=0
            )
            back = dot(unperm[...], block).astype(BF)
            gath[d, :, :, :, col : col + tile] = back.reshape(2, 2, rows, tile)
        rd_copy(d).start()

    def join(d):
        rd_copy(d).wait_recv()
        part = gath[d, core, 1 - hi].astype(F32) + dbuf[d, 1 - hi].astype(F32)
        sums[d, 1 - hi] = part.astype(BF)
        ry_copy(d).start()

    def near_join(d):
        rd_copy(d).wait_recv()
        for h in range(2):
            part = (gath[d, core, h].astype(F32) + dbuf[d, h].astype(F32)).astype(BF)
            if d == 0:
                retn[h, 0] = part
            else:
                sums[d, h] = part
        if d > 0:
            near_copy(d).start()

    def finish(d):
        ry_copy(d).wait_recv()
        total = gath[d, core, hi].astype(F32) + dbuf[d, hi].astype(F32)
        sums[d, hi] = (total + ybuf[d - lot].astype(F32)).astype(BF)
        rz_copy(d).start()

    def hand_over(d):
        y_copy(d).wait_recv()
        d_copy(d).start()

    def near_hand_over(d):
        z_copy(d).wait_recv()
        n_copy(d).wait_recv()
        d_copy(d).start()

    def near_sum():
        near_pick = combiner(next_slot, next_share, 0, lot)
        for d in range(1, lot):
            near_copy(d).wait_recv()
        for col in range(0, width, tile):
            near = retn[1 - hi, :, :, col : col + tile].reshape(lot * rows, tile)
            total = dot(near_pick[0], near) + dot(near_pick[1], near)
            nsend[:, col : col + tile] = total.astype(BF)
        for i in range(2):
            mix_y(i).start()

    near_order = list(range(2, lot)) + [1]
    att_y(0).start()
    att_y(1).start()
    for copy in weights:
        copy.wait()
    hand_over(far(0))
    arrange(far(0), 0)
    run(0, group)
    split(far(0), 0, True)
    for d in range(1, lot):
        near_hand_over(d)
    arrange(0, 0)
    join(far(0))
    forward(far(1))
    for d in range(1, lot):
        arrange(d, d * group)
    run(0, lot * group, 0, 2)
    run(0, lot * group, 2, 3)
    forward(far(2))
    finish(far(0))
    run(0, lot * group, 3, 4)
    for d in near_order:
        split(d, d * group, False)
    hand_over(far(1))
    split(0, 0, False)
    forward(far(3))
    for d in near_order:
        near_join(d)
    att_y(2).start()
    att_y(3).start()
    arrange(far(1), 0)
    hand_over(far(2))
    near_join(0)
    arrange(far(2), group)
    run(0, 2 * group)
    hand_over(far(3))
    split(far(1), 0, True)
    split(far(2), group, True)
    arrange(far(3), 0)
    join(far(1))
    join(far(2))
    run(0, group, 0, 2)
    finish(far(1))
    run(0, group, 2, 4)
    split(far(3), 0, True)
    finish(far(2))
    join(far(3))
    near_sum()
    finish(far(3))

    half = lot // 2
    own_near = combiner(own_slot, own_share, 0, lot)
    own_late = combiner(own_slot, own_share, lot, lot + half)
    own_early = combiner(own_slot, own_share, lot + half, ep)
    for i in range(half):
        rz_copy(far(i)).wait_recv()
    for col in range(0, width, tile):
        near = retn[hi, :, :, col : col + tile].reshape(lot * rows, tile)
        early = retx[half:, :, col : col + tile].reshape(half * rows, tile)
        total = dot(own_near[0], near) + dot(own_near[1], near)
        total = total + dot(own_early[0], early) + dot(own_early[1], early)
        partial[:, col : col + tile] = total
    for i in range(pieces):
        att_y(i).wait_recv()
    whole = pbuf[core, hi].astype(F32) + abuf[hi].astype(F32) + arecv[...].astype(F32)
    attended[...] = whole.astype(BF)
    for i in range(half, lot):
        rz_copy(far(i)).wait_recv()
    for i in range(2):
        mix_y(i).wait_recv()
    for col in range(0, width, tile):
        late = retx[:half, :, col : col + tile].reshape(half * rows, tile)
        total = partial[:, col : col + tile] + nrecv[:, col : col + tile].astype(F32)
        total = total + dot(own_late[0], late) + dot(own_late[1], late)
        mixed[:, col : col + tile] = total.astype(BF)

    @pl.when(me < ep - 1)
    def _():
        k_halo.wait_send()
        v_halo.wait_send()

    for copy in [routes_y, logits_y, tok_y, att_d, mix_y(0), mix_y(1)] + [att_y(i) for i in range(pieces)]:
        copy.wait_send()
    for d in range(ep):
        rd_copy(d).wait_send()
        if d > 0:
            z_copy(d).wait_send()
        if 0 < d < lot:
            n_copy(d).wait_send()
            near_copy(d).wait_send()
        if d >= lot:
            ry_copy(d).wait_send()
            rz_copy(d).wait_send()


def run_fused(dims, tok, gain, routes, logits, sink, qgain, kgain, streams):
    ep, local, cap, rows, width, ffn, own, seq, kv_heads, q_heads, experts = dims
    lot = ep // 2
    order = np.arange(local * 4 * cap)
    e, t, c = order // (4 * cap), order // cap % 4, order % cap
    perm = (t * rows + e * cap + c)[:, None] == np.arange(4 * rows)[None, :]
    perm = jnp.asarray(perm, BF)
    dma = pltpu.SemaphoreType.DMA
    vm = pl.BlockSpec(memory_space=pltpu.VMEM)
    anys = pl.BlockSpec(memory_space=pl.ANY)
    kv_width = kv_heads * 64

    def held(*shape, dtype=BF):
        return pltpu.VMEM(shape, dtype)

    return pl.pallas_call(
        lambda *refs: fused_kernel(dims, *refs),
        name="fused_layer",
        out_shape=(
            jax.ShapeDtypeStruct((own, width), BF), jax.ShapeDtypeStruct((own, width), BF)
        ),
        in_specs=[anys] * 16,
        out_specs=(vm, vm),
        scratch_shapes=[
            held(own, width), held(1, width, dtype=F32),
            held(2, own, dtype=jnp.int32), held(2, own, dtype=F32),
            pltpu.SMEM((1, q_heads), F32),
            held(q_heads, 64, dtype=F32), held(kv_heads, 64, dtype=F32),
            held(4 * rows, 4 * rows), held(4 * rows, 4 * rows),
            held(q_heads // 2, 128, dtype=F32),
            held(local, width, ffn), held(local, width, ffn), held(local, ffn, width),
            held(q_heads * 64, width),
            held(seq, q_heads * 64),
            held(seq + WINDOW, kv_width), held(seq + WINDOW, kv_width),
            held(kv_heads, seq + WINDOW, 128), held(kv_heads, seq + WINDOW, 128),
            held(seq, q_heads * 64),
            held(ep, rows, width), held(lot, rows, width),
            held(own, width), held(2, own, dtype=jnp.int32), held(2, own, dtype=F32), held(own, width),
            held(ep, 2, 2, rows, width),
            held(local, lot * 4 * cap, width),
            held(ep, 2, rows, width), held(ep, 2, rows, width),
            held(lot, rows, width),
            held(2, lot, rows, width), held(lot, rows, width),
            held(own, width), held(own, width),
            held(2, 2, own, width), held(2, own, width), held(own, width), held(own, width),
            held(own, width, dtype=F32),
            dma((16,)),
            dma((ep,)), dma((ep,)),
            dma((lot,)), dma((lot,)),
            dma((lot,)), dma((lot,)),
            dma((ep,)), dma((ep,)),
            dma((ep,)), dma((ep,)),
            dma((lot,)), dma((lot,)),
            dma((ep,)), dma((ep,)),
            dma((12,)), dma((12,)),
        ],
        compiler_params=pltpu.CompilerParams(
            collective_id=0, has_side_effects=True, vmem_limit_bytes=VMEM_LIMIT
        ),
    )(tok, gain, routes, logits, sink, qgain, kgain, perm, perm.T, *streams)


def hand_out(first, second):
    count = 2
    rows, width = first.shape
    piece = rows // count

    def kernel(first_in, second_in, first_out, second_out, held, sem_in, sem_out):
        pairs = ((first_in, first_out), (second_in, second_out))
        steps = [(a, i) for a in range(2) for i in range(count)]

        def inward(a, i):
            at = pl.ds(i * piece, piece)
            return pltpu.make_async_copy(pairs[a][0].at[at], held.at[a, at], sem_in.at[a, i])

        def outward(a, i):
            at = pl.ds(i * piece, piece)
            return pltpu.make_async_copy(held.at[a, at], pairs[a][1].at[at], sem_out.at[a, i])

        for step in steps:
            inward(*step).start()
        for step in steps:
            inward(*step).wait()
            outward(*step).start()
        for step in steps:
            outward(*step).wait()

    anys = pl.BlockSpec(memory_space=pl.ANY)
    shape = jax.ShapeDtypeStruct(first.shape, first.dtype)
    return pl.pallas_call(
        kernel,
        name="hand_out",
        out_shape=(shape, shape),
        in_specs=[anys, anys],
        out_specs=(anys, anys),
        scratch_shapes=[
            pltpu.VMEM((2, rows, width), BF),
            pltpu.SemaphoreType.DMA((2, count)),
            pltpu.SemaphoreType.DMA((2, count)),
        ],
    )(first, second)


def fits(dims, tp, kv_size):
    ep, local, cap, rows, width, ffn, own, seq, kv_heads, q_heads, experts = dims
    if tp != 4 or ep < 4 or ep & (ep - 1) or rows % 16 or cap % 4 or kv_size != 64:
        return False
    if own != 128 or seq != 4 * own or kv_heads % 2 or q_heads != 3 * kv_heads or width % 512:
        return False
    lot = ep // 2
    held = 3 * local * width * ffn + q_heads * 64 * width + 3 * seq * q_heads * 64
    held += rows * width * (11 * ep + 5 * lot) + local * lot * 4 * cap * width + 16 * own * width
    return 2 * held < 63 * 1024 * 1024


def on_device(
    query_rows,
    key_rows,
    value_rows,
    query_gain,
    key_gain,
    sink_logits,
    out_weight,
    expert_input,
    expert_gain,
    routes,
    route_logits,
    gate_weight,
    up_weight,
    down_weight,
):
    own_rows = expert_input.shape[0]
    fanout = routes.shape[1]
    capacity = (3 * own_rows * fanout + 2 * EXPERTS - 1) // (2 * EXPERTS)
    ep_size = lax.axis_size("ep")
    tp_size = lax.axis_size("tp")
    local_experts = gate_weight.shape[0]
    key_heads, head_size = key_gain.shape
    dims = (
        ep_size, local_experts, capacity, local_experts * capacity, expert_input.shape[1],
        gate_weight.shape[2], own_rows, query_rows.shape[0], key_heads, query_gain.shape[0],
        EXPERTS,
    )
    if fits(dims, tp_size, head_size):
        results = run_fused(
            dims, expert_input, expert_gain.reshape(1, -1), routes.T, route_logits.T,
            sink_logits.reshape(1, -1), query_gain, key_gain,
            (query_rows, key_rows, value_rows, out_weight, gate_weight, up_weight, down_weight),
        )
        return hand_out(*results)
    heads_out = attend(query_rows, key_rows, value_rows, query_gain, key_gain, sink_logits)
    projected = jnp.dot(heads_out, out_weight, preferred_element_type=jnp.float32).astype(
        jnp.bfloat16
    )
    widened = expert_input.astype(jnp.float32)
    normed = (
        widened
        * lax.rsqrt(jnp.mean(widened * widened, axis=-1, keepdims=True) + EPSILON)
        * expert_gain
    ).astype(jnp.bfloat16)
    route_weight = jax.nn.softmax(route_logits, axis=-1)
    attended = lax.psum_scatter(projected, "tp", scatter_dimension=0, tiled=True)
    combine = combine_matrix(routes, route_weight, capacity)
    sender = dispatch_matrix(routes, capacity)
    slot_rows = jnp.einsum(
        "ecr,rd->ecd", sender, normed, preferred_element_type=jnp.float32
    ).astype(jnp.bfloat16)
    slot_rows = slot_rows.reshape(ep_size, local_experts, capacity, -1)
    arrived = lax.all_to_all(slot_rows, "ep", split_axis=0, concat_axis=0, tiled=True)
    hidden_units = expert_hidden(
        lax.all_gather(arrived, "tp", axis=0, tiled=True), gate_weight, up_weight
    )
    partial_value = jnp.einsum(
        "aecf,efd->aecd", hidden_units, down_weight, preferred_element_type=jnp.float32
    ).astype(jnp.bfloat16)
    partial_value = partial_value.reshape(tp_size, ep_size * local_experts * capacity, -1)
    pieces = lax.all_to_all(partial_value, "tp", split_axis=0, concat_axis=0, tiled=True)
    summed = jnp.sum(pieces, axis=0, dtype=jnp.float32).astype(jnp.bfloat16)
    summed = summed.reshape(ep_size, local_experts * capacity, -1)
    returned = lax.all_to_all(summed, "ep", split_axis=0, concat_axis=0, tiled=True).reshape(
        EXPERTS, capacity, -1
    )
    expert_mix = jnp.einsum(
        "rec,ecd->rd", combine, returned.astype(jnp.float32), precision=lax.Precision.HIGHEST
    ).astype(jnp.bfloat16)
    return (attended, expert_mix)


def solution(mesh):
    placed = (
        P("ep", "tp"),
        P("ep", "tp"),
        P("ep", "tp"),
        P("tp", None),
        P("tp", None),
        P("tp"),
        P("tp", None),
        P(("ep", "tp"), None),
        P(),
        P(("ep", "tp"), None),
        P(("ep", "tp"), None),
        P("ep", None, "tp"),
        P("ep", None, "tp"),
        P("ep", "tp", None),
    )
    return jax.shard_map(
        on_device,
        mesh=mesh,
        in_specs=placed,
        out_specs=(P(("ep", "tp"), None), P(("ep", "tp"), None)),
        check_vma=False,
    )
```
